32 devices in a mesh: sp: 8 (over z, y), tp: 4 (over x, core).
Axes of the slice: x: 2, y: 2, z: 4, core: 2. Of those that a mesh axis runs over, the one named last changes fastest.
Arguments:
- tokens: bfloat16 [1024, 2048], P(('sp', 'tp')), may hold values from -8.5 to 8.5
- norm_gain: bfloat16 [2048], replicated, may hold values from 0.099609375 to 1.8984375
- w_query: bfloat16 [2048, 1024], P(None, 'tp'), may hold values from -0.088388348 to 0.088388348
- w_key: bfloat16 [2048, 512], P(None, 'tp'), may hold values from -5.3298174 to 5.3298174
- w_value: bfloat16 [2048, 512], P(None, 'tp'), may hold values from -0.125 to 0.125
- w_conv_value: bfloat16 [2048, 1024], P(None, 'tp'), may hold values from -0.125 to 0.125
- w_conv_gate: bfloat16 [2048, 1024], P(None, 'tp'), may hold values from -0.125 to 0.125
- conv_taps: bfloat16 [31, 1024], P(None, 'tp'), may hold values from -1 to 1
- conv_gain: bfloat16 [1024], P('tp'), may hold values from 0.099609375 to 1.8984375
- conv_bias: bfloat16 [1024], P('tp'), may hold values from -3 to 3
- cum_gate: float32 [1024, 8], P(None, 'tp'), may hold values from -125 to 0, as said below
- w_out_att: bfloat16 [1024, 2048], P('tp', 'sp'), may hold values from -0.28125 to 0.28125
- w_out_conv: bfloat16 [1024, 2048], P('tp', 'sp'), may hold values from -0.1875 to 0.1875
Outputs:
- mixed_out: bfloat16 [1024, 2048], P('sp', 'tp')
The draws below stay inside these ranges and needn't reach their ends.
Inputs may be any that keep to these rules, and one draw needn't show every extreme that they name: `cum_gate`: in each head, non-increasing along positions, and at most 0.
All inputs are finite; a program needn't handle non-finite values.
Results may differ from the reference program's by a relative error of at most 0.012.
Values may be sent and summed in bfloat16 or wider, within the bound.
A program may use at most 64 MiB of HBM per device.

```python
import math
import jax
import jax.numpy as jnp
from jax import lax

D = 2048
ASKER_HEAD_TALLY = 8
KV_HEADS = 4
HEAD = 128
CONV = 1024
KW = 31
TOK_DEV = 128
SERIES_ENTRIES = 1024


def draw_tokens(key, part):
    starting_number = jax.random.fold_in(key, 37)
    noise_key, direction_key, orientation_key = jax.random.split(starting_number, 3)
    noise = jax.random.truncated_normal(noise_key, -4.0, 4.0, (SERIES_ENTRIES, D), jnp.float32)
    direction = jax.random.truncated_normal(direction_key, -3.0, 3.0, (D,), jnp.float32)
    orientation = jnp.where(jax.random.bernoulli(orientation_key), 1.0, -1.0)
    places = jnp.arange(SERIES_ENTRIES, dtype=jnp.float32)
    drift_line = 1.5 * orientation * (2.0 * places / (SERIES_ENTRIES - 1) - 1.0)
    return (noise + drift_line[:, None] * direction[None, :]).astype(jnp.bfloat16)


def query_key_pair(key):
    starting_number = jax.random.fold_in(key, 11)
    first_key = jax.random.fold_in(starting_number, 0)
    second_key = jax.random.fold_in(starting_number, 1)
    mixing_key = jax.random.fold_in(starting_number, 3)
    scale = D ** (-0.5)
    weight_query = jax.random.truncated_normal(first_key, -4.0, 4.0, (D, ASKER_HEAD_TALLY * HEAD), jnp.float32) * scale
    weight_key = jax.random.truncated_normal(second_key, -4.0, 4.0, (D, KV_HEADS * HEAD), jnp.float32) * scale
    grouped = weight_query.reshape(D, KV_HEADS, ASKER_HEAD_TALLY // KV_HEADS, HEAD).sum(axis=2).reshape(D, KV_HEADS * HEAD)
    mixing = jax.random.uniform(mixing_key, (KV_HEADS,), jnp.float32, -0.7, -0.4)
    mixing_columns = jnp.repeat(mixing, HEAD)
    mixed = grouped * mixing_columns[None, :] + weight_key
    weight_key = mixed
    return (weight_query, weight_key)


def draw_w_query(key, part):
    return query_key_pair(key)[0].astype(jnp.bfloat16)


def draw_w_key(key, part):
    return query_key_pair(key)[1].astype(jnp.bfloat16)


def draw_cum_gate(key, part):
    starting_number = jax.random.fold_in(key, 23)
    shuffle_seed_handle, quick_seed_handle, gradual_seed_handle, tile_seed_handle, coarse_seed_handle, spurt_seed_handle, channelwise_seed_handle = jax.random.split(starting_number, 7)
    ranks = jnp.argsort(jax.random.permutation(shuffle_seed_handle, ASKER_HEAD_TALLY))
    fast_heads = ranks < ASKER_HEAD_TALLY // 2
    fast_rate = jnp.exp(jax.random.uniform(quick_seed_handle, (ASKER_HEAD_TALLY,), jnp.float32, math.log(1.0 / 100.0), math.log(1.0 / 30.0)))
    slow_total = jax.random.uniform(gradual_seed_handle, (ASKER_HEAD_TALLY,), jnp.float32, 0.2, 0.4)
    rate = jnp.where(fast_heads, fast_rate, slow_total / SERIES_ENTRIES)
    block_factor = jnp.exp(jax.random.uniform(tile_seed_handle, (SERIES_ENTRIES // TOK_DEV, ASKER_HEAD_TALLY), jnp.float32, math.log(0.5), math.log(2.0)))
    block_factor = jnp.repeat(block_factor, TOK_DEV, axis=0)
    rough = jax.random.uniform(coarse_seed_handle, (SERIES_ENTRIES, ASKER_HEAD_TALLY), jnp.float32, 0.2, 1.8)
    iteration_tally = -rate[None, :] * block_factor * rough
    spot_number = jax.random.randint(spurt_seed_handle, (2, ASKER_HEAD_TALLY), 0, SERIES_ENTRIES)
    objective_number = jax.random.uniform(channelwise_seed_handle, (2, ASKER_HEAD_TALLY), jnp.float32, 0.2, 0.35)
    location_number = jnp.arange(SERIES_ENTRIES, dtype=jnp.int32)
    for spurt_extent in range(2):
        match_selector = location_number[:, None] == spot_number[spurt_extent][None, :]
        iteration_tally = iteration_tally + jnp.where(match_selector, jnp.log(1.0 - objective_number[spurt_extent])[None, :], 0.0)
    return jnp.cumsum(iteration_tally, axis=0).astype(jnp.float32)


def block_levels(own_key, shape, cuts, low, largest):
    factor_of, own = 1.0, jax.random.fold_in(own_key, 6)
    for dim, shards_of in cuts:
        draws = jnp.exp(jax.random.uniform(jax.random.fold_in(own, dim), (shards_of,), jnp.float32, low / len(cuts), largest / len(cuts)))
        factor_of = factor_of * jnp.repeat(draws, shape[dim] // shards_of).reshape([-1 if axis == dim else 1 for axis in range(len(shape))])
    return factor_of


def centred(key, shape, deviation, limit, shards=(), held_as=jnp.bfloat16):
    entries = deviation * jax.random.normal(key, shape, jnp.float32)
    if shards:
        entries = entries * block_levels(key, shape, shards, -0.22, 0.18)
    return jnp.clip(entries, -limit, limit).astype(held_as)


def setup_inputs(seed: int = 0) -> dict:
    key_of = jax.random.split(jax.random.key(seed), 14)
    return {
        "tokens": draw_tokens(jax.random.fold_in(key_of[13], 71), 0),
        "norm_gain": jnp.clip(1.0 + 0.18 * jax.random.normal(key_of[1], (D,), jnp.float32), 0.099609375, 1.8984375).astype(jnp.bfloat16),
        "w_query": draw_w_query(jax.random.fold_in(key_of[13], 71), 0),
        "w_key": draw_w_key(jax.random.fold_in(key_of[13], 71), 0),
        "w_value": centred(key_of[4], (D, KV_HEADS * HEAD), D ** -0.5, 0.125, ((1, 4),)),
        "w_conv_value": centred(key_of[5], (D, CONV), D ** -0.5, 0.125, ((1, 4),)),
        "w_conv_gate": centred(key_of[6], (D, CONV), D ** -0.5, 0.125, ((1, 4),)),
        "conv_taps": centred(key_of[7], (KW, CONV), KW ** -0.5, 1.0, ((1, 4),)),
        "conv_gain": jnp.clip(1.0 + 0.18 * jax.random.normal(key_of[8], (CONV,), jnp.float32), 0.099609375, 1.8984375).astype(jnp.bfloat16),
        "conv_bias": centred(key_of[9], (CONV,), 0.5, 3.0, ((0, 4),)),
        "cum_gate": draw_cum_gate(jax.random.fold_in(key_of[13], 71), 0),
        "w_out_att": centred(key_of[11], (ASKER_HEAD_TALLY * HEAD, D), (1.5 / (ASKER_HEAD_TALLY * HEAD) ** 0.5), 0.28125, ((0, 4), (1, 8))),
        "w_out_conv": centred(key_of[12], (CONV, D), CONV ** -0.5, 0.1875, ((0, 4), (1, 8))),
    }


def reference(tokens, norm_gain, w_query, w_key, w_value, w_conv_value, w_conv_gate, conv_taps, conv_gain, conv_bias, cum_gate, w_out_att, w_out_conv):
    floats = tokens.astype(jnp.float32)
    normed = (floats * lax.rsqrt(lax.optimization_barrier(jnp.mean(floats * floats, axis=-1, keepdims=True)) + 1e-06) * norm_gain.astype(jnp.float32)).astype(jnp.bfloat16)
    query = jnp.dot(normed, w_query, preferred_element_type=jnp.float32).astype(jnp.bfloat16)
    key_rows = jnp.dot(normed, w_key, preferred_element_type=jnp.float32).astype(jnp.bfloat16)
    value_rows = jnp.dot(normed, w_value, preferred_element_type=jnp.float32).astype(jnp.bfloat16)
    group_size = ASKER_HEAD_TALLY // KV_HEADS
    query_heads = query.astype(jnp.float32).reshape(SERIES_ENTRIES, ASKER_HEAD_TALLY, HEAD)
    key_heads = jnp.repeat(key_rows.astype(jnp.float32).reshape(SERIES_ENTRIES, KV_HEADS, HEAD), group_size, axis=1)
    value_heads = jnp.repeat(value_rows.astype(jnp.float32).reshape(SERIES_ENTRIES, KV_HEADS, HEAD), group_size, axis=1)
    block_rows = math.gcd(SERIES_ENTRIES, 256)
    scale = 1.0 / math.sqrt(HEAD)
    gates_by_head = cum_gate.T
    key_places = jnp.arange(SERIES_ENTRIES, dtype=jnp.int32)

    def one_block(index):
        first = (index * block_rows).astype(jnp.int32)
        query_block = lax.dynamic_slice_in_dim(query_heads, first, block_rows, 0)
        gate_block = lax.dynamic_slice_in_dim(cum_gate, first, block_rows, 0)
        scores = jnp.einsum('thd,shd->hts', query_block, key_heads) * scale
        logits = scores + gate_block.T[:, :, None] - gates_by_head[:, None, :]
        query_places = first + jnp.arange(block_rows, dtype=jnp.int32)
        allowed = key_places[None, :] <= query_places[:, None]
        logits = jnp.where(allowed[None], logits, -jnp.inf)
        row_max = lax.optimization_barrier(jnp.max(logits, axis=-1, keepdims=True))
        weights = jnp.where(allowed[None], jnp.exp(logits - row_max), 0.0)
        denom = lax.optimization_barrier(jnp.sum(weights, axis=-1))
        rounded = lax.optimization_barrier(weights.astype(jnp.bfloat16)).astype(jnp.float32)
        numer = jnp.einsum('hts,shd->htd', rounded, value_heads)
        return (numer / denom[:, :, None]).astype(jnp.bfloat16)
    blocks = lax.map(one_block, jnp.arange(SERIES_ENTRIES // block_rows, dtype=jnp.int32))
    attended = jnp.transpose(blocks, (0, 2, 1, 3)).reshape(SERIES_ENTRIES, ASKER_HEAD_TALLY * HEAD)
    value_part = jnp.dot(normed, w_conv_value, preferred_element_type=jnp.float32)
    gate_part = jnp.dot(normed, w_conv_gate, preferred_element_type=jnp.float32)
    glu = (value_part * jax.nn.sigmoid(gate_part)).astype(jnp.bfloat16)
    padded = jnp.concatenate([jnp.zeros((KW - 1, CONV), jnp.bfloat16), glu], axis=0).astype(jnp.float32)
    taps = conv_taps.astype(jnp.float32)
    conv = jnp.zeros((SERIES_ENTRIES, CONV), jnp.float32)
    for shift_tap in range(KW):
        conv = conv + taps[shift_tap][None, :] * padded[shift_tap:shift_tap + SERIES_ENTRIES]
    mean_c = lax.optimization_barrier(jnp.mean(conv, axis=-1, keepdims=True))
    var_c = lax.optimization_barrier(jnp.mean(conv * conv, axis=-1, keepdims=True)) - mean_c * mean_c
    shaped = (conv - mean_c) * lax.rsqrt(var_c + 1e-05) * conv_gain.astype(jnp.float32) + conv_bias.astype(jnp.float32)
    conv_act = jax.nn.silu(shaped).astype(jnp.bfloat16)
    total = jnp.dot(attended, w_out_att, preferred_element_type=jnp.float32) + jnp.dot(conv_act, w_out_conv, preferred_element_type=jnp.float32)
    return total.astype(jnp.bfloat16)
```

```python
import functools
import math

import jax
import jax.numpy as jnp
from jax import lax
from jax.experimental import pallas as pl
from jax.experimental.pallas import tpu as pltpu
from jax.sharding import PartitionSpec as P

HEAD = 128
CONV = 1024
KW = 31


def shifted(array, axis, by):
    peers = lax.axis_size(axis)
    pairs = [(i, i + by) for i in range(peers) if 0 <= i + by < peers]
    return lax.ppermute(array, axis, pairs)


def shards(
    tokens,
    norm_gain,
    w_query,
    w_key,
    w_value,
    w_conv_value,
    w_conv_gate,
    conv_taps,
    conv_gain,
    conv_bias,
    cum_gate,
    w_out_att,
    w_out_conv,
):
    query_cols = w_query.shape[1]
    kv_cols = w_key.shape[1]
    conv_cols = w_conv_value.shape[1]
    head_count = query_cols // HEAD
    kv_count = kv_cols // HEAD
    group_size = head_count // kv_count
    gain_float = norm_gain.astype(jnp.float32)
    floats = lax.all_gather(tokens, "tp", axis=0, tiled=True).astype(jnp.float32)
    normed = (
        floats * lax.rsqrt(jnp.mean(floats * floats, axis=-1, keepdims=True) + 1e-06) * gain_float
    ).astype(jnp.bfloat16)
    query_part = jnp.dot(normed, w_query, preferred_element_type=jnp.float32).astype(jnp.bfloat16)
    key_part = jnp.dot(normed, w_key, preferred_element_type=jnp.float32).astype(jnp.bfloat16)
    value_part = jnp.dot(normed, w_value, preferred_element_type=jnp.float32).astype(jnp.bfloat16)
    value_glu = jnp.dot(normed, w_conv_value, preferred_element_type=jnp.float32)
    gate_glu = jnp.dot(normed, w_conv_gate, preferred_element_type=jnp.float32)
    glu_part = (value_glu * jax.nn.sigmoid(gate_glu)).astype(jnp.bfloat16)
    joined = jnp.concatenate([query_part, key_part, value_part, glu_part], axis=1)
    local_rows = joined.shape[0]
    query = joined[:, :query_cols]
    key_rows = joined[:, query_cols : query_cols + kv_cols]
    value_rows = joined[:, query_cols + kv_cols : query_cols + 2 * kv_cols]
    glu = joined[:, query_cols + 2 * kv_cols :]
    offset = lax.axis_index("sp") * local_rows
    query_places = offset + jnp.arange(local_rows, dtype=jnp.int32)
    query_gate = lax.dynamic_slice_in_dim(cum_gate, offset, local_rows, 0).T
    query_groups = query.reshape(local_rows, kv_count, group_size, HEAD)
    scale = 1.0 / math.sqrt(HEAD)

    def attend_block(state, key_block, value_block, key_start):
        run_max, run_sum, run_acc = state
        span = key_block.shape[0]
        key_heads = key_block.reshape(span, kv_count, HEAD)
        value_heads = value_block.reshape(span, kv_count, HEAD)
        scores = (
            jnp.einsum(
                "tkgd,skd->kgts", query_groups, key_heads, preferred_element_type=jnp.float32
            ).reshape(head_count, local_rows, span)
            * scale
        )
        key_gate = lax.dynamic_slice_in_dim(cum_gate, key_start, span, 0).T
        logits = scores + query_gate[:, :, None] - key_gate[:, None, :]
        key_places = key_start + jnp.arange(span, dtype=jnp.int32)
        allowed = (key_places[None, :] <= query_places[:, None])[None]
        logits = jnp.where(allowed, logits, -1e30)
        new_max = jnp.maximum(run_max, jnp.max(logits, axis=-1))
        weights = jnp.where(allowed, jnp.exp(logits - new_max[:, :, None]), 0.0)
        factor = jnp.exp(run_max - new_max)
        new_sum = run_sum * factor + jnp.sum(weights, axis=-1)
        grouped = weights.astype(jnp.bfloat16).reshape(kv_count, group_size, local_rows, span)
        product = jnp.einsum(
            "kgts,skd->kgtd", grouped, value_heads, preferred_element_type=jnp.float32
        ).reshape(head_count, local_rows, HEAD)
        new_acc = run_acc * factor[:, :, None] + product
        return (new_max, new_sum, new_acc)

    shard_rows = key_rows.shape[0]

    def fold_keys(state, pieces, start):
        key_piece, value_piece = pieces
        span = key_piece.shape[0]
        shards_in = span // shard_rows
        group = 1
        for divisor in range(1, shards_in + 1):
            if shards_in % divisor == 0 and divisor * shard_rows <= 2048:
                group = divisor
        block = group * shard_rows
        if block >= span:
            return attend_block(state, key_piece, value_piece, start)
        key_blocks = key_piece.reshape(span // block, block, kv_cols)
        value_blocks = value_piece.reshape(span // block, block, kv_cols)
        firsts = start + block * jnp.arange(span // block, dtype=jnp.int32)

        def step_block(inner, items):
            return (attend_block(inner, items[0], items[1], items[2]), None)

        result, unused = lax.scan(step_block, state, (key_blocks, value_blocks, firsts))
        return result

    start_state = (
        jnp.full((head_count, local_rows), -1e30, jnp.float32),
        jnp.zeros((head_count, local_rows), jnp.float32),
        jnp.zeros((head_count, local_rows, HEAD), jnp.float32),
    )
    run_max, run_sum, run_acc = fold_keys(
        start_state,
        (
            lax.all_gather(key_rows, "sp", axis=0, tiled=True),
            lax.all_gather(value_rows, "sp", axis=0, tiled=True),
        ),
        jnp.int32(0),
    )
    attended = jnp.transpose(
        (run_acc / run_sum[:, :, None]).astype(jnp.bfloat16), (1, 0, 2)
    ).reshape(local_rows, query_cols)
    rim = shifted(glu[local_rows - (KW - 1) :], "sp", 1)
    padded = jnp.concatenate([rim, glu], axis=0).astype(jnp.float32)
    taps = conv_taps.astype(jnp.float32)
    conv = jnp.zeros((local_rows, conv_cols), jnp.float32)
    for shift_tap in range(KW):
        conv = conv + taps[shift_tap][None, :] * padded[shift_tap : shift_tap + local_rows]
    first_sum, square_sum = lax.psum((jnp.sum(conv, axis=1), jnp.sum(conv * conv, axis=1)), "tp")
    mean_c = (first_sum / CONV)[:, None]
    var_c = (square_sum / CONV)[:, None] - mean_c * mean_c
    shaped = (conv - mean_c) * lax.rsqrt(var_c + 1e-05) * conv_gain.astype(
        jnp.float32
    ) + conv_bias.astype(jnp.float32)
    conv_act = jax.nn.silu(shaped).astype(jnp.bfloat16)
    att_weight, conv_weight = (
        lax.all_gather(w_out_att, "sp", axis=1, tiled=True),
        lax.all_gather(w_out_conv, "sp", axis=1, tiled=True),
    )
    terms = jnp.dot(attended, att_weight, preferred_element_type=jnp.float32) + jnp.dot(
        conv_act, conv_weight, preferred_element_type=jnp.float32
    )
    return lax.psum_scatter(terms.astype(jnp.bfloat16), "tp", scatter_dimension=1, tiled=True)


F32 = jnp.float32
BF16 = jnp.bfloat16


def fused_kernel(
    n_sp,
    n_tp,
    tokens_h,
    gain_h,
    wq_h,
    wk_h,
    wv_h,
    wcv_h,
    wcg_h,
    taps_h,
    cgain_h,
    cbias_h,
    gate_h,
    woa_h,
    woc_h,
    out_r,
    tok,
    normed,
    wq,
    wk,
    wv,
    wcv,
    wcg,
    taps,
    gate,
    gain_v,
    cgain_v,
    cbias_v,
    wbuf,
    kv,
    pad,
    rim_out,
    rim_in,
    stat,
    act,
    pair_out,
    pair_in,
    cross_out,
    cross_in,
    local_sem,
    tok_send,
    tok_recv,
    w_send,
    w_recv,
    kv_send,
    kv_recv,
    rim_sem,
    stat_send,
    stat_recv,
    out_send,
    out_recv,
):
    s = lax.axis_index("sp")
    t = lax.axis_index("tp")
    rem = lax.rem
    core = t + 1 - 2 * rem(t, 2)
    cross = rem(t + 2, n_tp)
    diag = rem(core + 2, n_tp)
    side = s + 1 - 2 * rem(s, 2)
    up = rem(s + 2, n_sp)
    down = rem(s + n_sp - 2, n_sp)
    after = rem(s + 1, n_sp)
    other = rem(s + n_sp - 1 + 2 * rem(s, 2), n_sp)

    rows_in = tokens_h.shape[0]
    rows = rows_in * n_tp
    head_count = gate_h.shape[0]
    ccols = wcv_h.shape[1]
    half = woa_h.shape[0]

    def local(src, dst, index):
        copy = pltpu.make_async_copy(src, dst, local_sem.at[index])
        copy.start()
        return copy

    def remote(src, dst, send, recv, where):
        return pltpu.make_async_remote_copy(
            src_ref=src,
            dst_ref=dst,
            send_sem=send,
            recv_sem=recv,
            device_id=where,
            device_id_type=pl.DeviceIdType.MESH,
        )

    own_tok = local(tokens_h, tok.at[t], 0)
    own_a = local(woa_h, wbuf.at[s, pl.ds(0, half)], 1)
    own_b = local(woc_h, wbuf.at[s, pl.ds(half, half)], 2)
    load_gate = local(gate_h, gate, 3)
    load_k = local(wk_h, wk, 4)
    load_v = local(wv_h, wv, 5)
    load_cv = local(wcv_h, wcv, 6)
    load_cg = local(wcg_h, wcg, 7)
    load_q = local(wq_h, wq, 8)
    load_taps = local(taps_h, taps, 9)
    load_gain = local(gain_h, gain_v, 10)
    load_cgain = local(cgain_h, cgain_v, 11)
    load_cbias = local(cbias_h, cbias_v, 12)

    barrier = pltpu.get_barrier_semaphore()
    greeted = [{"tp": core}, {"tp": cross}, {"tp": diag}]
    greeted += [{"sp": side}, {"sp": up}, {"sp": down}, {"sp": other}]
    for peer in greeted:
        pl.semaphore_signal(
            barrier, inc=1, device_id=peer, device_id_type=pl.DeviceIdType.MESH
        )
    own_tok.wait()
    pl.semaphore_wait(barrier, len(greeted))

    sent = []

    def go(copy, when=None):
        if when is None:
            copy.start()
        else:
            pl.when(when)(copy.start)
        sent.append((copy, when))

    def tok_copy(slot, number, where):
        return remote(tok.at[slot], tok.at[slot], tok_send.at[number], tok_recv.at[slot], where)

    go(tok_copy(t, 0, {"tp": cross}))
    go(tok_copy(t, 1, {"tp": core}))

    z = s // 2
    last = n_sp // 2 - 1

    def w_copy(slot, part, number, where):
        piece = wbuf.at[slot, pl.ds(part * half, half)]
        return remote(piece, piece, w_send.at[number], w_recv.at[slot, part], where)

    def kv_copy(slot, part, number, where):
        piece = kv.at[part, pl.ds(pl.multiple_of(slot * rows, rows), rows)]
        return remote(piece, piece, kv_send.at[number], kv_recv.at[slot, part], where)

    class Gather:
        def __init__(self, copy_of, both_ways):
            self.copy_of, self.both, self.count = copy_of, both_ways, 0

        def send(self, slot, part, where, when=None):
            go(self.copy_of(slot, part, self.count, {"sp": where}), when)
            self.count += 1

        def wait(self, slot, part, when=None):
            copy = self.copy_of(slot, part, 0, {"sp": side})
            if when is None:
                copy.wait_recv()
            else:
                pl.when(when)(copy.wait_recv)

        def own(self):
            for part in range(2):
                self.send(s, part, up, z < last)
                if self.both:
                    self.send(s, part, down, z > 0)
                self.send(s, part, side)

        def pass_on(self, distance, part):
            below = rem(s + n_sp - 2 * distance, n_sp)
            above = rem(s + 2 * distance, n_sp)
            self.wait(below, part, z >= distance)
            self.send(below, part, up, (z >= distance) & (z < last))
            if distance > 1 or part == 0:
                self.send(below, part, side, z >= distance)
            if self.both:
                self.wait(above, part, z + distance <= last)
                self.send(above, part, down, (z + distance <= last) & (z > 0))
                if distance > 1 or part == 0:
                    self.send(above, part, side, z + distance <= last)
            if distance == 1:
                self.wait(side, part)
                if part == 1:
                    self.send(side, part, up, z < last)
                    if self.both:
                        self.send(side, part, down, z > 0)

        def end(self):
            for distance in range(1, last + 1):
                for part in range(2):
                    self.wait(rem(side + n_sp - 2 * distance, n_sp), part, z >= distance)
                    if self.both:
                        self.wait(
                            rem(side + 2 * distance, n_sp), part, z + distance <= last
                        )

    w_gather = Gather(w_copy, True)
    kv_gather = Gather(kv_copy, False)

    own_a.wait()
    own_b.wait()
    w_gather.own()
    for later in range(1, last + 1):

        @pl.when(later > z)
        def _():
            blank = pl.ds(later * 2 * rows, 2 * rows)
            kv[:, blank, :] = jnp.zeros((2, 2 * rows, kv.shape[2]), BF16)


    diagonal = lax.broadcasted_iota(jnp.int32, (rows, rows), 0) == lax.broadcasted_iota(
        jnp.int32, (rows, rows), 1
    )

    def to_lanes(column):
        return jnp.sum(jnp.where(diagonal, column, 0.0), axis=0, keepdims=True)

    def to_sublanes(row):
        return jnp.sum(jnp.where(diagonal, row, 0.0), axis=1, keepdims=True)

    load_gain.wait()
    gain = gain_v[...].astype(F32)[None, :]

    def norm_rows(slot):
        floats = tok[slot].astype(F32)
        scaled = floats * lax.rsqrt(jnp.mean(floats * floats, axis=-1, keepdims=True) + 1e-06)
        normed[pl.ds(pl.multiple_of(slot * rows_in, rows_in), rows_in), :] = (
            scaled * gain
        ).astype(BF16)

    norm_rows(t)
    tok_copy(core, 0, {"tp": core}).wait_recv()
    norm_rows(core)
    tok_copy(cross, 0, {"tp": core}).wait_recv()
    go(tok_copy(cross, 2, {"tp": core}))
    norm_rows(cross)
    tok_copy(diag, 0, {"tp": core}).wait_recv()
    norm_rows(diag)

    def project(weight):
        return jnp.dot(normed[...], weight[...], preferred_element_type=F32)

    own_rows = pl.ds(pl.multiple_of(s * rows, rows), rows)
    load_k.wait()
    load_v.wait()
    kv[0, own_rows, :] = project(wk).astype(BF16)
    kv[1, own_rows, :] = project(wv).astype(BF16)
    kv_gather.own()
    w_gather.pass_on(1, 0)

    load_cv.wait()
    load_cg.wait()
    glu = (project(wcv) * jax.nn.sigmoid(project(wcg))).astype(BF16)
    rim = rim_out.shape[0]
    rim_out[...] = glu[rows - rim :]
    rim_copy = remote(rim_out, rim_in, rim_sem.at[0], rim_sem.at[1], {"sp": after})
    go(rim_copy)
    pad[pl.ds(rim, rows), :] = glu.astype(F32)

    kv_gather.pass_on(1, 0)
    kv_gather.pass_on(1, 1)
    w_gather.pass_on(1, 1)

    for part in range(2):
        kv_gather.pass_on(2, part)
    for part in range(2):
        w_gather.pass_on(2, part)
    load_q.wait()
    query = project(wq).astype(BF16)

    load_taps.wait()
    rim_copy.wait_recv()
    pad[pl.ds(0, rim), :] = jnp.where(s == 0, 0.0, rim_in[...].astype(F32))
    lead = rim - (KW - 1)
    conv = jnp.zeros((rows, ccols), F32)
    for tap in range(KW):
        conv = conv + taps[pl.ds(tap, 1), :].astype(F32) * pad[pl.ds(lead + tap, rows), :]
    stat[t] = jnp.zeros(stat.shape[1:], F32)
    stat[t, pl.ds(0, 1), :] = to_lanes(jnp.sum(conv, axis=1, keepdims=True))
    stat[t, pl.ds(1, 1), :] = to_lanes(jnp.sum(conv * conv, axis=1, keepdims=True))

    def stat_copy(slot, number, where):
        return remote(stat.at[slot], stat.at[slot], stat_send.at[number], stat_recv.at[slot], where)

    for number, peer in enumerate((core, cross, diag)):
        go(stat_copy(t, number, {"tp": peer}))


    load_cgain.wait()
    load_cbias.wait()
    for peer in (core, cross, diag):
        stat_copy(peer, 0, {"tp": core}).wait_recv()
    totals = stat[0]
    for peer in range(1, n_tp):
        totals = totals + stat[peer]
    channels = n_tp * ccols
    mean_c = to_sublanes(totals[0:1]) / channels
    var_c = to_sublanes(totals[1:2]) / channels - mean_c * mean_c
    shaped = (conv - mean_c) * lax.rsqrt(var_c + 1e-05) * cgain_v[...].astype(F32)[
        None, :
    ] + cbias_v[...].astype(F32)[None, :]
    act[:, pl.ds(half, ccols)] = (shaped / (1.0 + jnp.exp(-shaped))).astype(BF16)

    for part in range(2):
        kv_gather.pass_on(3, part)
    kv_gather.end()
    for part in range(2):
        w_gather.pass_on(3, part)
    length = kv.shape[1]
    scale = 1.0 / math.sqrt(HEAD)
    key_places = lax.broadcasted_iota(jnp.int32, (rows, length), 1)
    allowed = key_places <= s * rows + lax.broadcasted_iota(jnp.int32, (rows, length), 0)
    load_gate.wait()
    for head in range(head_count):
        scores = (
            lax.dot_general(
                query[:, head * HEAD : (head + 1) * HEAD],
                kv[0],
                (((1,), (1,)), ((), ())),
                preferred_element_type=F32,
            )
            * scale
        )
        query_gate = to_sublanes(gate[pl.ds(head, 1), own_rows])
        logits = scores + query_gate - gate[pl.ds(head, 1), :]
        logits = jnp.where(allowed, logits, -1e30)
        weights = jnp.exp(logits - jnp.max(logits, axis=-1, keepdims=True))
        denom = jnp.sum(weights, axis=-1, keepdims=True)
        numer = jnp.dot(weights.astype(BF16), kv[1], preferred_element_type=F32)
        act[:, pl.ds(head * HEAD, HEAD)] = (numer / denom).astype(BF16)

    w_gather.end()

    per = n_sp // n_tp
    wide = wbuf.shape[2]

    def terms(chunk, block):
        return jnp.dot(act[...], wbuf[chunk * per + block], preferred_element_type=F32)

    x = t // 2
    for step, column in enumerate((1 - x, x)):
        chunk = 2 * column + rem(core, 2)
        for block in range(per):
            pair_out[step, :, pl.ds(block * wide, wide)] = terms(chunk, block).astype(BF16)
        go(
            remote(
                pair_out.at[step],
                pair_in.at[step],
                out_send.at[step],
                out_recv.at[step],
                {"tp": core},
            )
        )
    mine = [terms(2 * (1 - x) + rem(t, 2), block) for block in range(per)]
    remote(
        pair_out.at[0], pair_in.at[0], out_send.at[0], out_recv.at[0], {"tp": core}
    ).wait_recv()
    for block in range(per):
        piece = pl.ds(block * wide, wide)
        cross_out[:, piece] = (mine[block] + pair_in[0, :, piece].astype(F32)).astype(BF16)
    cross_copy = remote(cross_out, cross_in, out_send.at[2], out_recv.at[2], {"tp": cross})
    go(cross_copy)
    mine = [terms(t, block) for block in range(per)]
    remote(
        pair_out.at[1], pair_in.at[1], out_send.at[1], out_recv.at[1], {"tp": core}
    ).wait_recv()
    for block in range(per):
        mine[block] = mine[block] + pair_in[1, :, pl.ds(block * wide, wide)].astype(F32)
    cross_copy.wait_recv()
    for block in range(per):
        piece = pl.ds(block * wide, wide)
        out_r[:, piece] = (mine[block] + cross_in[:, piece].astype(F32)).astype(BF16)
    for copy, when in sent:
        if when is None:
            copy.wait_send()
        else:
            pl.when(when)(copy.wait_send)


def fused(n_sp, n_tp, *args):
    tokens, gain, wq, wk, wv, wcv, wcg, taps, cgain, cbias, gate, woa, woc = args
    rows_in, width = tokens.shape
    rows = rows_in * n_tp
    rim = -(-(KW - 1) // 16) * 16
    wide = woa.shape[1]
    out_wide = wide * n_sp // n_tp
    both = woa.shape[0] + woc.shape[0]
    hbm = pl.BlockSpec(memory_space=pltpu.HBM)
    vmem = pl.BlockSpec(memory_space=pltpu.VMEM)
    dma = pltpu.SemaphoreType.DMA
    scratch = [
        pltpu.VMEM((n_tp, rows_in, width), BF16),
        pltpu.VMEM((rows, width), BF16),
        *[pltpu.VMEM(w.shape, w.dtype) for w in (wq, wk, wv, wcv, wcg, taps)],
        pltpu.VMEM(gate.shape[::-1], F32),
        pltpu.VMEM(gain.shape, BF16),
        pltpu.VMEM(cgain.shape, BF16),
        pltpu.VMEM(cbias.shape, BF16),
        pltpu.VMEM((n_sp, both, wide), BF16),
        pltpu.VMEM((2, n_sp * rows, wk.shape[1]), BF16),
        pltpu.VMEM((rim + rows, wcv.shape[1]), F32),
        pltpu.VMEM((rim, wcv.shape[1]), BF16),
        pltpu.VMEM((rim, wcv.shape[1]), BF16),
        pltpu.VMEM((n_tp, 8, rows), F32),
        pltpu.VMEM((rows, both), BF16),
        pltpu.VMEM((2, rows, out_wide), BF16),
        pltpu.VMEM((2, rows, out_wide), BF16),
        pltpu.VMEM((rows, out_wide), BF16),
        pltpu.VMEM((rows, out_wide), BF16),
        dma((13,)),
        dma((3,)),
        dma((n_tp,)),
        dma((40,)),
        dma((n_sp, 2)),
        dma((40,)),
        dma((n_sp, 2)),
        dma((2,)),
        dma((3,)),
        dma((n_tp,)),
        dma((3,)),
        dma((3,)),
    ]
    return pl.pallas_call(
        functools.partial(fused_kernel, n_sp, n_tp),
        out_shape=pltpu.VMEM((rows, out_wide), BF16),
        in_specs=[hbm] * 13,
        out_specs=vmem,
        scratch_shapes=scratch,
        compiler_params=pltpu.CompilerParams(
            collective_id=0, has_side_effects=True, vmem_limit_bytes=66_846_720
        ),
    )(
        tokens, gain, wq, wk, wv, wcv, wcg, taps,
        cgain, cbias, gate.T, woa, woc,
    )


def layer(sizes, *args):
    n_sp, n_tp = sizes["sp"], sizes["tp"]
    tokens, wq, wk, wcv, woa, woc = (args[k] for k in (0, 2, 3, 5, 11, 12))
    fits = (
        n_sp == 8
        and n_tp == 4
        and tokens.shape[0] * n_tp == HEAD
        and wk.shape[1] == HEAD
        and woa.shape[1] % HEAD == 0
        and woa.shape == woc.shape
        and wq.shape[1] == wcv.shape[1] == woa.shape[0]
    )
    if fits:
        return fused(n_sp, n_tp, *args)
    return shards(*args)


def solution(mesh):
    return jax.shard_map(
        functools.partial(layer, dict(mesh.shape)),
        mesh=mesh,
        in_specs=(
            P(("sp", "tp"), None),
            P(),
            P(None, "tp"),
            P(None, "tp"),
            P(None, "tp"),
            P(None, "tp"),
            P(None, "tp"),
            P(None, "tp"),
            P("tp"),
            P("tp"),
            P(None, "tp"),
            P("tp", "sp"),
            P("tp", "sp"),
        ),
        out_specs=P("sp", "tp"),
        check_vma=False,
    )
```

```python
import functools
import math

import jax
import jax.numpy as jnp
from jax import lax
from jax.experimental import pallas as pl
from jax.experimental.pallas import tpu as pltpu
from jax.sharding import PartitionSpec as P

HEAD = 128
CONV = 1024
KW = 31


def shifted(array, axis, by):
    peers = lax.axis_size(axis)
    pairs = [(i, i + by) for i in range(peers) if 0 <= i + by < peers]
    return lax.ppermute(array, axis, pairs)


def shards(
    tokens,
    norm_gain,
    w_query,
    w_key,
    w_value,
    w_conv_value,
    w_conv_gate,
    conv_taps,
    conv_gain,
    conv_bias,
    cum_gate,
    w_out_att,
    w_out_conv,
):
    query_cols = w_query.shape[1]
    kv_cols = w_key.shape[1]
    conv_cols = w_conv_value.shape[1]
    head_count = query_cols // HEAD
    kv_count = kv_cols // HEAD
    group_size = head_count // kv_count
    gain_float = norm_gain.astype(jnp.float32)
    floats = lax.all_gather(tokens, "tp", axis=0, tiled=True).astype(jnp.float32)
    normed = (
        floats * lax.rsqrt(jnp.mean(floats * floats, axis=-1, keepdims=True) + 1e-06) * gain_float
    ).astype(jnp.bfloat16)
    query_part = jnp.dot(normed, w_query, preferred_element_type=jnp.float32).astype(jnp.bfloat16)
    key_part = jnp.dot(normed, w_key, preferred_element_type=jnp.float32).astype(jnp.bfloat16)
    value_part = jnp.dot(normed, w_value, preferred_element_type=jnp.float32).astype(jnp.bfloat16)
    value_glu = jnp.dot(normed, w_conv_value, preferred_element_type=jnp.float32)
    gate_glu = jnp.dot(normed, w_conv_gate, preferred_element_type=jnp.float32)
    glu_part = (value_glu * jax.nn.sigmoid(gate_glu)).astype(jnp.bfloat16)
    joined = jnp.concatenate([query_part, key_part, value_part, glu_part], axis=1)
    local_rows = joined.shape[0]
    query = joined[:, :query_cols]
    key_rows = joined[:, query_cols : query_cols + kv_cols]
    value_rows = joined[:, query_cols + kv_cols : query_cols + 2 * kv_cols]
    glu = joined[:, query_cols + 2 * kv_cols :]
    offset = lax.axis_index("sp") * local_rows
    query_places = offset + jnp.arange(local_rows, dtype=jnp.int32)
    query_gate = lax.dynamic_slice_in_dim(cum_gate, offset, local_rows, 0).T
    query_groups = query.reshape(local_rows, kv_count, group_size, HEAD)
    scale = 1.0 / math.sqrt(HEAD)

    def attend_block(state, key_block, value_block, key_start):
        run_max, run_sum, run_acc = state
        span = key_block.shape[0]
        key_heads = key_block.reshape(span, kv_count, HEAD)
        value_heads = value_block.reshape(span, kv_count, HEAD)
        scores = (
            jnp.einsum(
                "tkgd,skd->kgts", query_groups, key_heads, preferred_element_type=jnp.float32
            ).reshape(head_count, local_rows, span)
            * scale
        )
        key_gate = lax.dynamic_slice_in_dim(cum_gate, key_start, span, 0).T
        logits = scores + query_gate[:, :, None] - key_gate[:, None, :]
        key_places = key_start + jnp.arange(span, dtype=jnp.int32)
        allowed = (key_places[None, :] <= query_places[:, None])[None]
        logits = jnp.where(allowed, logits, -1e30)
        new_max = jnp.maximum(run_max, jnp.max(logits, axis=-1))
        weights = jnp.where(allowed, jnp.exp(logits - new_max[:, :, None]), 0.0)
        factor = jnp.exp(run_max - new_max)
        new_sum = run_sum * factor + jnp.sum(weights, axis=-1)
        grouped = weights.astype(jnp.bfloat16).reshape(kv_count, group_size, local_rows, span)
        product = jnp.einsum(
            "kgts,skd->kgtd", grouped, value_heads, preferred_element_type=jnp.float32
        ).reshape(head_count, local_rows, HEAD)
        new_acc = run_acc * factor[:, :, None] + product
        return (new_max, new_sum, new_acc)

    shard_rows = key_rows.shape[0]

    def fold_keys(state, pieces, start):
        key_piece, value_piece = pieces
        span = key_piece.shape[0]
        shards_in = span // shard_rows
        group = 1
        for divisor in range(1, shards_in + 1):
            if shards_in % divisor == 0 and divisor * shard_rows <= 2048:
                group = divisor
        block = group * shard_rows
        if block >= span:
            return attend_block(state, key_piece, value_piece, start)
        key_blocks = key_piece.reshape(span // block, block, kv_cols)
        value_blocks = value_piece.reshape(span // block, block, kv_cols)
        firsts = start + block * jnp.arange(span // block, dtype=jnp.int32)

        def step_block(inner, items):
            return (attend_block(inner, items[0], items[1], items[2]), None)

        result, unused = lax.scan(step_block, state, (key_blocks, value_blocks, firsts))
        return result

    start_state = (
        jnp.full((head_count, local_rows), -1e30, jnp.float32),
        jnp.zeros((head_count, local_rows), jnp.float32),
        jnp.zeros((head_count, local_rows, HEAD), jnp.float32),
    )
    run_max, run_sum, run_acc = fold_keys(
        start_state,
        (
            lax.all_gather(key_rows, "sp", axis=0, tiled=True),
            lax.all_gather(value_rows, "sp", axis=0, tiled=True),
        ),
        jnp.int32(0),
    )
    attended = jnp.transpose(
        (run_acc / run_sum[:, :, None]).astype(jnp.bfloat16), (1, 0, 2)
    ).reshape(local_rows, query_cols)
    rim = shifted(glu[local_rows - (KW - 1) :], "sp", 1)
    padded = jnp.concatenate([rim, glu], axis=0).astype(jnp.float32)
    taps = conv_taps.astype(jnp.float32)
    conv = jnp.zeros((local_rows, conv_cols), jnp.float32)
    for shift_tap in range(KW):
        conv = conv + taps[shift_tap][None, :] * padded[shift_tap : shift_tap + local_rows]
    first_sum, square_sum = lax.psum((jnp.sum(conv, axis=1), jnp.sum(conv * conv, axis=1)), "tp")
    mean_c = (first_sum / CONV)[:, None]
    var_c = (square_sum / CONV)[:, None] - mean_c * mean_c
    shaped = (conv - mean_c) * lax.rsqrt(var_c + 1e-05) * conv_gain.astype(
        jnp.float32
    ) + conv_bias.astype(jnp.float32)
    conv_act = jax.nn.silu(shaped).astype(jnp.bfloat16)
    att_weight, conv_weight = (
        lax.all_gather(w_out_att, "sp", axis=1, tiled=True),
        lax.all_gather(w_out_conv, "sp", axis=1, tiled=True),
    )
    terms = jnp.dot(attended, att_weight, preferred_element_type=jnp.float32) + jnp.dot(
        conv_act, conv_weight, preferred_element_type=jnp.float32
    )
    return lax.psum_scatter(terms.astype(jnp.bfloat16), "tp", scatter_dimension=1, tiled=True)


F32 = jnp.float32
BF16 = jnp.bfloat16


def fused_kernel(
    n_sp,
    n_tp,
    tokens_h,
    gain_h,
    wq_h,
    wk_h,
    wv_h,
    wcv_h,
    wcg_h,
    taps_h,
    cgain_h,
    cbias_h,
    gate_h,
    woa_h,
    woc_h,
    out_r,
    tok,
    normed,
    wq,
    wk,
    wv,
    wcv,
    wcg,
    taps,
    gate,
    gain_v,
    cgain_v,
    cbias_v,
    wbuf,
    kv,
    pad,
    rim_out,
    rim_in,
    stat,
    act,
    acc,
    pair_out,
    pair_in,
    sum_out,
    sum_in,
    local_sem,
    tok_send,
    tok_recv,
    w_send,
    w_recv,
    kv_send,
    kv_recv,
    rim_sem,
    stat_send,
    stat_recv,
    act_send,
    act_recv,
    pair_send,
    pair_recv,
    sum_send,
    sum_recv,
):
    scope = jax.named_scope
    s = lax.axis_index("sp")
    t = lax.axis_index("tp")
    rem = lax.rem
    last = n_sp // 2 - 1
    core = t + 1 - 2 * rem(t, 2)
    cross = rem(t + 2, n_tp)
    diag = rem(core + 2, n_tp)
    y = rem(s, 2)
    z = s // 2
    side = s + 1 - 2 * y
    mate = (z + 1 - 2 * rem(z, 2)) * 2 + y
    far = (last - z) * 2 + y
    after = rem(s + 1, n_sp)
    up = rem(s + 2, n_sp)
    up_two = rem(s + 4, n_sp)
    home = (t == z) | (t == last - z)
    near_mine = rem(t, 2) == rem(z, 2)

    rows_in = tokens_h.shape[0]
    rows = rows_in * n_tp
    head_count = gate_h.shape[0]
    ccols = wcv_h.shape[1]
    half = woa_h.shape[0]
    wide = wbuf.shape[2]
    pieces = w_recv.shape[1]
    deep = wbuf.shape[1] // pieces

    def local(src, dst, index):
        copy = pltpu.make_async_copy(src, dst, local_sem.at[index])
        copy.start()
        return copy

    def remote(src, dst, send, recv, where):
        return pltpu.make_async_remote_copy(
            src_ref=src,
            dst_ref=dst,
            send_sem=send,
            recv_sem=recv,
            device_id=where,
            device_id_type=pl.DeviceIdType.MESH,
        )

    own_tok = local(tokens_h, tok.at[t], 0)
    own_a = local(woa_h, wbuf.at[y, pl.ds(0, half)], 1)
    own_b = local(woc_h, wbuf.at[y, pl.ds(half, half)], 2)
    load_gate = local(gate_h, gate, 3)
    load_gain = local(gain_h, gain_v, 10)
    load_k = local(wk_h, wk, 4)
    load_v = local(wv_h, wv, 5)
    load_cv = local(wcv_h, wcv, 6)
    load_cg = local(wcg_h, wcg, 7)
    load_q = local(wq_h, wq, 8)
    load_taps = local(taps_h, taps, 9)
    load_cgain = local(cgain_h, cgain_v, 11)
    load_cbias = local(cbias_h, cbias_v, 12)

    with scope("barrier"):
        barrier = pltpu.get_barrier_semaphore()
        greeted = [{"tp": core}, {"tp": cross}, {"tp": diag}, {"sp": mate, "tp": cross}]
        greeted += [{"sp": rem(s + by, n_sp)} for by in range(1, n_sp)]
        for peer in greeted:
            pl.semaphore_signal(
                barrier, inc=1, device_id=peer, device_id_type=pl.DeviceIdType.MESH
            )
        own_tok.wait()
        pl.semaphore_wait(barrier, len(greeted))

    sent = []

    def go(copy, when=None):
        if when is None:
            copy.start()
        else:
            pl.when(when)(copy.start)
        sent.append((copy, when))

    tok_half = rows_in // 2

    def tok_copy(slot, part, number, where):
        piece = tok.at[slot, pl.ds(part * tok_half, tok_half)]
        return remote(piece, piece, tok_send.at[number], tok_recv.at[slot, part], where)

    for part in range(2):
        go(tok_copy(t, part, part, {"tp": cross}))
    for part in range(2):
        go(tok_copy(t, part, 2 + part, {"tp": core}))

    def w_copy(source, target, piece, number, where):
        span = pl.ds(piece * deep, deep)
        return remote(
            wbuf.at[source, span],
            wbuf.at[target, span],
            w_send.at[number],
            w_recv.at[target, piece],
            where,
        )

    w_count = [0]

    def w_go(source, target, piece, where, when=None):
        number = w_count[0]
        w_count[0] += 1
        go(w_copy(source, target, piece, number, {"sp": where}), when)

    def w_far(first, past, when=None):
        for piece in range(first, past):
            w_go(y, 2 + y, piece, far, when)

    def w_pass(first, past, when=True):
        for piece in range(first, past):
            pl.when(when)(w_copy(2 + y, 2 + y, piece, 0, {"sp": side}).wait_recv)
            w_go(2 + y, 2 + y, piece, side, when)

    def w_wait(block):
        for piece in range(pieces):
            w_copy(2 * block + 1 - y, 2 * block + 1 - y, piece, 0, {"sp": side}).wait_recv()

    own_a.wait()
    own_b.wait()
    w_far(0, 1)
    w_far(1, pieces - 1, z != 1)
    w_far(pieces - 1, pieces, z > last // 2)
    for piece in range(pieces):
        w_go(y, y, piece, side)

    @pl.when(y == 0)
    def _():
        kv[:, pl.ds(pl.multiple_of(side * rows, rows), rows), :] = jnp.zeros(
            (2, rows, kv.shape[2]), BF16
        )

    diagonal = lax.broadcasted_iota(jnp.int32, (rows, rows), 0) == lax.broadcasted_iota(
        jnp.int32, (rows, rows), 1
    )

    def to_lanes(column):
        return jnp.sum(jnp.where(diagonal, column, 0.0), axis=0, keepdims=True)

    def to_sublanes(row):
        return jnp.sum(jnp.where(diagonal, row, 0.0), axis=1, keepdims=True)

    load_gain.wait()
    gain = gain_v[...].astype(F32)[None, :]

    def norm_rows(slot):
        floats = tok[slot].astype(F32)
        scaled = floats * lax.rsqrt(jnp.mean(floats * floats, axis=-1, keepdims=True) + 1e-06)
        normed[pl.ds(pl.multiple_of(slot * rows_in, rows_in), rows_in), :] = (
            scaled * gain
        ).astype(BF16)

    def tok_wait(slot):
        for part in range(2):
            tok_copy(slot, part, 0, {"tp": core}).wait_recv()

    with scope("norm0"):
        norm_rows(t)
    with scope("tokw1"):
        tok_wait(core)
    with scope("norm1"):
        norm_rows(core)
    with scope("tokw2"):
        for part in range(2):
            tok_copy(cross, part, 0, {"tp": core}).wait_recv()
            go(tok_copy(cross, part, 4 + part, {"tp": core}))
    with scope("norm2"):
        norm_rows(cross)
    with scope("tokw3"):
        tok_wait(diag)
    with scope("norm3"):
        norm_rows(diag)

    def project(weight):
        return jnp.dot(normed[...], weight[...], preferred_element_type=F32)

    own_rows = pl.ds(pl.multiple_of(s * rows, rows), rows)
    kv_count = [0]

    def kv_go(slot, part, where, when):
        piece = kv.at[part, pl.ds(pl.multiple_of(slot * rows, rows), rows)]
        number = kv_count[0]
        kv_count[0] += 1
        go(
            remote(piece, piece, kv_send.at[number], kv_recv.at[slot, part], {"sp": where}),
            when,
        )

    def kv_wait(slot, part, when):
        piece = kv.at[part, pl.ds(pl.multiple_of(slot * rows, rows), rows)]
        copy = remote(piece, piece, kv_send.at[0], kv_recv.at[slot, part], {"sp": side})
        pl.when(when)(copy.wait_recv)

    def kv_pass(distance, part, when):
        slot = rem(s + n_sp - 2 * distance, n_sp)
        kv_wait(slot, part, when)
        if distance < last:
            kv_go(slot, part, up, when & (z == last - 1))
        kv_go(slot, part, side, when)

    with scope("projkv"):
        load_k.wait()
        load_v.wait()
        for part, weight in enumerate((wk, wv)):
            kv[part, own_rows, :] = project(weight).astype(BF16)
            kv_go(s, part, up, z < last)
            kv_go(s, part, up_two, z == 0)
            kv_go(s, part, side, y == 0)
    rim = rim_out.shape[0]
    with scope("glu"):
        load_cv.wait()
        load_cg.wait()
        glu = (project(wcv) * jax.nn.sigmoid(project(wcg))).astype(BF16)
        rim_out[...] = glu[rows - rim :]
    rim_copy = remote(rim_out, rim_in, rim_sem.at[0], rim_sem.at[1], {"sp": after})
    go(rim_copy)
    with scope("projq"):
        pad[pl.ds(rim, rows), :] = glu.astype(F32)
        load_q.wait()
        query = project(wq).astype(BF16)
    w_pass(0, 1, z == last)
    with scope("kvp1"):
        for part in range(2):
            kv_pass(1, part, z >= 1)
        for part in range(2):
            kv_pass(2, part, z == last - 1)
    w_pass(1, 2, z == last)
    with scope("rimw"):
        load_taps.wait()
        rim_copy.wait_recv()
    with scope("conv"):
        pad[pl.ds(0, rim), :] = jnp.where(s == 0, 0.0, rim_in[...].astype(F32))
        lead = rim - (KW - 1)
        conv = jnp.zeros((rows, ccols), F32)
        for tap in range(KW):
            conv = conv + taps[pl.ds(tap, 1), :].astype(F32) * pad[pl.ds(lead + tap, rows), :]
        stat[t] = jnp.zeros(stat.shape[1:], F32)
        stat[t, pl.ds(0, 1), :] = to_lanes(jnp.sum(conv, axis=1, keepdims=True))
        stat[t, pl.ds(1, 1), :] = to_lanes(jnp.sum(conv * conv, axis=1, keepdims=True))

    def stat_copy(slot, number, where):
        return remote(stat.at[slot], stat.at[slot], stat_send.at[number], stat_recv.at[slot], where)

    for number, peer in enumerate((core, cross, diag)):
        go(stat_copy(t, number, {"tp": peer}))
    w_far(1, pieces, z == 1)
    with scope("kvp2"):
        for part in range(2):
            kv_pass(2, part, z == last)
    with scope("wp0"):
        w_pass(0, 1, z < last)
        w_pass(1, pieces, z <= last // 2)
        w_pass(2, pieces - 1, z == last)
    def act_copy(first, size, number):
        span = pl.ds(first, size)
        return remote(
            act.at[0, :, span],
            act.at[1, :, span],
            act_send.at[number],
            act_recv.at[number],
            {"sp": mate},
        )

    act_copies = [act_copy(half, ccols, 0)]
    act_copies += [act_copy(head * HEAD, HEAD, 1 + head) for head in range(head_count)]

    def attend(layer):
        for distance in range(layer + 1):
            for part in range(2):
                slot = rem(side + n_sp - 2 * distance, n_sp)
                kv_wait(slot, part, True if distance else y == 1)
        length = 2 * (layer + 1) * rows
        scale = 1.0 / math.sqrt(HEAD)
        key_places = lax.broadcasted_iota(jnp.int32, (rows, length), 1)
        allowed = key_places <= s * rows + lax.broadcasted_iota(jnp.int32, (rows, length), 0)
        load_gate.wait()
        for head in range(head_count):
            scores = (
                lax.dot_general(
                    query[:, head * HEAD : (head + 1) * HEAD],
                    kv[0, pl.ds(0, length)],
                    (((1,), (1,)), ((), ())),
                    preferred_element_type=F32,
                )
                * scale
            )
            query_gate = to_sublanes(gate[pl.ds(head, 1), own_rows])
            logits = scores + query_gate - gate[pl.ds(head, 1), pl.ds(0, length)]
            logits = jnp.where(allowed, logits, -1e30)
            weights = jnp.exp(logits - jnp.max(logits, axis=-1, keepdims=True))
            denom = jnp.sum(weights, axis=-1, keepdims=True)
            numer = jnp.dot(
                weights.astype(BF16), kv[1, pl.ds(0, length)], preferred_element_type=F32
            )
            act[0, :, pl.ds(head * HEAD, HEAD)] = (numer / denom).astype(BF16)
            act_copies[1 + head].start()

    for layer in range(last):

        @pl.when(z == layer)
        def _():
            with scope("attn_early"):
                attend(layer)

    w_far(pieces - 1, pieces, z == 0)
    with scope("statw"):
        load_cgain.wait()
        load_cbias.wait()
        for peer in (core, cross, diag):
            stat_copy(peer, 0, {"tp": core}).wait_recv()

    with scope("convact"):
        totals = stat[0]
        for peer in range(1, n_tp):
            totals = totals + stat[peer]
        channels = n_tp * ccols
        mean_c = to_sublanes(totals[0:1]) / channels
        var_c = to_sublanes(totals[1:2]) / channels - mean_c * mean_c
        shaped = (conv - mean_c) * lax.rsqrt(var_c + 1e-05) * cgain_v[...].astype(F32)[
            None, :
        ] + cbias_v[...].astype(F32)[None, :]
        act[0, :, pl.ds(half, ccols)] = (shaped / (1.0 + jnp.exp(-shaped))).astype(BF16)
    go(act_copies[0])
    with scope("kvp3"):
        for part in range(2):
            kv_pass(3, part, z == last)
    @pl.when(z == last)
    def _():
        with scope("attn_late"):
            attend(last)

    sent.extend((copy, None) for copy in act_copies[1:])
    with scope("wp1"):
        w_pass(1, pieces, z == last - 1)
        w_pass(pieces - 1, pieces, z == last)
    with scope("wnear"):
        w_wait(0)

    def columns(part):
        return pl.ds(part * wide, wide)

    def product(row_set, block, part):
        return jnp.dot(
            act[row_set], wbuf[2 * block + part], preferred_element_type=F32
        )

    def pair_copy(row_set, part):
        return remote(
            pair_out.at[row_set, :, columns(part)],
            pair_in.at[row_set, :, columns(part)],
            pair_send.at[row_set, part],
            pair_recv.at[row_set, part],
            {"tp": core},
        )

    def ship(row_set, block):
        for part in range(2):
            pair_out[row_set, :, columns(part)] = product(row_set, block, part).astype(BF16)
            pair_copy(row_set, part).start()

    def keep(row_set, block):
        for part in range(2):
            acc[row_set, :, columns(part)] = product(row_set, block, part)

    def sum_copy(source, target, part, where):
        return remote(
            sum_out.at[source, :, columns(part)],
            sum_in.at[target, :, columns(part)],
            sum_send.at[source, part],
            sum_recv.at[target, part],
            where,
        )

    away = jnp.logical_not(home)
    own_sum = [sum_copy(0, 0, part, {"tp": cross}) for part in range(2)]
    mate_home = [sum_copy(1, 1, part, {"sp": mate}) for part in range(2)]
    mate_away = [sum_copy(1, 0, part, {"sp": mate, "tp": cross}) for part in range(2)]

    def finish(row_set):
        for part in range(2):
            pair_copy(row_set, part).wait_recv()
            total = acc[row_set, :, columns(part)] + pair_in[row_set, :, columns(part)].astype(F32)
            if row_set == 0:
                acc[0, :, columns(part)] = total
            sum_out[row_set, :, columns(part)] = total.astype(BF16)
            if row_set == 0:
                pl.when(away)(own_sum[part].start)
            else:
                pl.when(home)(mate_home[part].start)
                pl.when(away)(mate_away[part].start)

    def mate_wait():
        for copy in act_copies:
            copy.wait_recv()

    @pl.when(near_mine)
    def _():
        with scope("a_near0"):
            keep(0, 0)
        with scope("a_mate"):
            mate_wait()
        with scope("a_near1"):
            keep(1, 0)
        with scope("a_fin1"):
            finish(1)
        with scope("a_fin0"):
            finish(0)
        with scope("a_wfar"):
            w_wait(1)
        with scope("a_far"):
            ship(1, 1)
            ship(0, 1)

    @pl.when(jnp.logical_not(near_mine))
    def _():
        with scope("b_near0"):
            ship(0, 0)
        with scope("b_mate"):
            mate_wait()
        with scope("b_near1"):
            ship(1, 0)
        with scope("b_wfar"):
            w_wait(1)
        with scope("b_far"):
            keep(1, 1)
            keep(0, 1)
        with scope("b_fin1"):
            finish(1)
        with scope("b_fin0"):
            finish(0)

    @pl.when(home)
    def _():
        for part in range(2):
            with scope("c_home"):
                own_sum[part].wait_recv()
            span = columns(part)
            out_r[:, span] = (acc[0, :, span] + sum_in[0, :, span].astype(F32)).astype(BF16)

    @pl.when(away)
    def _():
        for part in range(2):
            with scope("c_away"):
                mate_home[part].wait_recv()
                mate_away[part].wait_recv()
            span = columns(part)
            out_r[:, span] = (
                sum_in[0, :, span].astype(F32) + sum_in[1, :, span].astype(F32)
            ).astype(BF16)

    for part in range(2):
        sent.extend((pair_copy(row_set, part), None) for row_set in range(2))
        sent.append((own_sum[part], away))
        sent.append((mate_home[part], None))
    with scope("sendw"):
        for copy, when in sent:
            if when is None:
                copy.wait_send()
            else:
                pl.when(when)(copy.wait_send)


def fused(n_sp, n_tp, *args):
    tokens, gain, wq, wk, wv, wcv, wcg, taps, cgain, cbias, gate, woa, woc = args
    rows_in, width = tokens.shape
    rows = rows_in * n_tp
    rim = -(-(KW - 1) // 16) * 16
    wide = woa.shape[1]
    out_wide = wide * n_sp // n_tp
    both = woa.shape[0] + woc.shape[0]
    pieces = 4
    heads = gate.shape[1]
    hbm = pl.BlockSpec(memory_space=pltpu.HBM)
    vmem = pl.BlockSpec(memory_space=pltpu.VMEM)
    dma = pltpu.SemaphoreType.DMA
    scratch = [
        pltpu.VMEM((n_tp, rows_in, width), BF16),
        pltpu.VMEM((rows, width), BF16),
        *[pltpu.VMEM(w.shape, w.dtype) for w in (wq, wk, wv, wcv, wcg, taps)],
        pltpu.VMEM(gate.shape[::-1], F32),
        pltpu.VMEM(gain.shape, BF16),
        pltpu.VMEM(cgain.shape, BF16),
        pltpu.VMEM(cbias.shape, BF16),
        pltpu.VMEM((4, both, wide), BF16),
        pltpu.VMEM((2, n_sp * rows, wk.shape[1]), BF16),
        pltpu.VMEM((rim + rows, wcv.shape[1]), F32),
        pltpu.VMEM((rim, wcv.shape[1]), BF16),
        pltpu.VMEM((rim, wcv.shape[1]), BF16),
        pltpu.VMEM((n_tp, 8, rows), F32),
        pltpu.VMEM((2, rows, both), BF16),
        pltpu.VMEM((2, rows, out_wide), F32),
        *[pltpu.VMEM((2, rows, out_wide), BF16)] * 4,
        dma((13,)),
        dma((6,)),
        dma((n_tp, 2)),
        dma((12 * pieces,)),
        dma((4, pieces)),
        dma((32,)),
        dma((n_sp, 2)),
        dma((2,)),
        dma((3,)),
        dma((n_tp,)),
        dma((1 + heads,)),
        dma((1 + heads,)),
        *[dma((2, 2))] * 4,
    ]
    result = pltpu.VMEM((rows, out_wide), BF16)
    spare = 3 * rows * out_wide
    return pl.pallas_call(
        functools.partial(fused_kernel, n_sp, n_tp),
        out_shape=result,
        in_specs=[hbm] * 13,
        out_specs=vmem,
        scratch_shapes=scratch,
        compiler_params=pltpu.CompilerParams(
            collective_id=0, has_side_effects=True, vmem_limit_bytes=67_043_328 - spare
        ),
    )(
        tokens, gain, wq, wk, wv, wcv, wcg, taps,
        cgain, cbias, gate.T, woa, woc,
    )


def layer(sizes, *args):
    n_sp, n_tp = sizes["sp"], sizes["tp"]
    tokens, wq, wk, wcv, woa, woc = (args[k] for k in (0, 2, 3, 5, 11, 12))
    fits = (
        n_sp == 8
        and n_tp == 4
        and tokens.shape[0] * n_tp == HEAD
        and wk.shape[1] == HEAD
        and woa.shape[1] % HEAD == 0
        and woa.shape == woc.shape
        and wq.shape[1] == wcv.shape[1] == woa.shape[0]
    )
    if fits:
        return fused(n_sp, n_tp, *args)
    return shards(*args)


def solution(mesh):
    return jax.shard_map(
        functools.partial(layer, dict(mesh.shape)),
        mesh=mesh,
        in_specs=(
            P(("sp", "tp"), None),
            P(),
            P(None, "tp"),
            P(None, "tp"),
            P(None, "tp"),
            P(None, "tp"),
            P(None, "tp"),
            P(None, "tp"),
            P("tp"),
            P("tp"),
            P(None, "tp"),
            P("tp", "sp"),
            P("tp", "sp"),
        ),
        out_specs=P("sp", "tp"),
        check_vma=False,
    )
```

```python
import functools
import math

import jax
import jax.numpy as jnp
from jax import lax
from jax.experimental import pallas as pl
from jax.experimental.pallas import tpu as pltpu
from jax.sharding import PartitionSpec as P

HEAD = 128
CONV = 1024
KW = 31


def shifted(array, axis, by):
    peers = lax.axis_size(axis)
    pairs = [(i, i + by) for i in range(peers) if 0 <= i + by < peers]
    return lax.ppermute(array, axis, pairs)


def shards(
    tokens,
    norm_gain,
    w_query,
    w_key,
    w_value,
    w_conv_value,
    w_conv_gate,
    conv_taps,
    conv_gain,
    conv_bias,
    cum_gate,
    w_out_att,
    w_out_conv,
):
    query_cols = w_query.shape[1]
    kv_cols = w_key.shape[1]
    conv_cols = w_conv_value.shape[1]
    head_count = query_cols // HEAD
    kv_count = kv_cols // HEAD
    group_size = head_count // kv_count
    gain_float = norm_gain.astype(jnp.float32)
    floats = lax.all_gather(tokens, "tp", axis=0, tiled=True).astype(jnp.float32)
    normed = (
        floats * lax.rsqrt(jnp.mean(floats * floats, axis=-1, keepdims=True) + 1e-06) * gain_float
    ).astype(jnp.bfloat16)
    query_part = jnp.dot(normed, w_query, preferred_element_type=jnp.float32).astype(jnp.bfloat16)
    key_part = jnp.dot(normed, w_key, preferred_element_type=jnp.float32).astype(jnp.bfloat16)
    value_part = jnp.dot(normed, w_value, preferred_element_type=jnp.float32).astype(jnp.bfloat16)
    value_glu = jnp.dot(normed, w_conv_value, preferred_element_type=jnp.float32)
    gate_glu = jnp.dot(normed, w_conv_gate, preferred_element_type=jnp.float32)
    glu_part = (value_glu * jax.nn.sigmoid(gate_glu)).astype(jnp.bfloat16)
    joined = jnp.concatenate([query_part, key_part, value_part, glu_part], axis=1)
    local_rows = joined.shape[0]
    query = joined[:, :query_cols]
    key_rows = joined[:, query_cols : query_cols + kv_cols]
    value_rows = joined[:, query_cols + kv_cols : query_cols + 2 * kv_cols]
    glu = joined[:, query_cols + 2 * kv_cols :]
    offset = lax.axis_index("sp") * local_rows
    query_places = offset + jnp.arange(local_rows, dtype=jnp.int32)
    query_gate = lax.dynamic_slice_in_dim(cum_gate, offset, local_rows, 0).T
    query_groups = query.reshape(local_rows, kv_count, group_size, HEAD)
    scale = 1.0 / math.sqrt(HEAD)

    def attend_block(state, key_block, value_block, key_start):
        run_max, run_sum, run_acc = state
        span = key_block.shape[0]
        key_heads = key_block.reshape(span, kv_count, HEAD)
        value_heads = value_block.reshape(span, kv_count, HEAD)
        scores = (
            jnp.einsum(
                "tkgd,skd->kgts", query_groups, key_heads, preferred_element_type=jnp.float32
            ).reshape(head_count, local_rows, span)
            * scale
        )
        key_gate = lax.dynamic_slice_in_dim(cum_gate, key_start, span, 0).T
        logits = scores + query_gate[:, :, None] - key_gate[:, None, :]
        key_places = key_start + jnp.arange(span, dtype=jnp.int32)
        allowed = (key_places[None, :] <= query_places[:, None])[None]
        logits = jnp.where(allowed, logits, -1e30)
        new_max = jnp.maximum(run_max, jnp.max(logits, axis=-1))
        weights = jnp.where(allowed, jnp.exp(logits - new_max[:, :, None]), 0.0)
        factor = jnp.exp(run_max - new_max)
        new_sum = run_sum * factor + jnp.sum(weights, axis=-1)
        grouped = weights.astype(jnp.bfloat16).reshape(kv_count, group_size, local_rows, span)
        product = jnp.einsum(
            "kgts,skd->kgtd", grouped, value_heads, preferred_element_type=jnp.float32
        ).reshape(head_count, local_rows, HEAD)
        new_acc = run_acc * factor[:, :, None] + product
        return (new_max, new_sum, new_acc)

    shard_rows = key_rows.shape[0]

    def fold_keys(state, pieces, start):
        key_piece, value_piece = pieces
        span = key_piece.shape[0]
        shards_in = span // shard_rows
        group = 1
        for divisor in range(1, shards_in + 1):
            if shards_in % divisor == 0 and divisor * shard_rows <= 2048:
                group = divisor
        block = group * shard_rows
        if block >= span:
            return attend_block(state, key_piece, value_piece, start)
        key_blocks = key_piece.reshape(span // block, block, kv_cols)
        value_blocks = value_piece.reshape(span // block, block, kv_cols)
        firsts = start + block * jnp.arange(span // block, dtype=jnp.int32)

        def step_block(inner, items):
            return (attend_block(inner, items[0], items[1], items[2]), None)

        result, unused = lax.scan(step_block, state, (key_blocks, value_blocks, firsts))
        return result

    start_state = (
        jnp.full((head_count, local_rows), -1e30, jnp.float32),
        jnp.zeros((head_count, local_rows), jnp.float32),
        jnp.zeros((head_count, local_rows, HEAD), jnp.float32),
    )
    run_max, run_sum, run_acc = fold_keys(
        start_state,
        (
            lax.all_gather(key_rows, "sp", axis=0, tiled=True),
            lax.all_gather(value_rows, "sp", axis=0, tiled=True),
        ),
        jnp.int32(0),
    )
    attended = jnp.transpose(
        (run_acc / run_sum[:, :, None]).astype(jnp.bfloat16), (1, 0, 2)
    ).reshape(local_rows, query_cols)
    rim = shifted(glu[local_rows - (KW - 1) :], "sp", 1)
    padded = jnp.concatenate([rim, glu], axis=0).astype(jnp.float32)
    taps = conv_taps.astype(jnp.float32)
    conv = jnp.zeros((local_rows, conv_cols), jnp.float32)
    for shift_tap in range(KW):
        conv = conv + taps[shift_tap][None, :] * padded[shift_tap : shift_tap + local_rows]
    first_sum, square_sum = lax.psum((jnp.sum(conv, axis=1), jnp.sum(conv * conv, axis=1)), "tp")
    mean_c = (first_sum / CONV)[:, None]
    var_c = (square_sum / CONV)[:, None] - mean_c * mean_c
    shaped = (conv - mean_c) * lax.rsqrt(var_c + 1e-05) * conv_gain.astype(
        jnp.float32
    ) + conv_bias.astype(jnp.float32)
    conv_act = jax.nn.silu(shaped).astype(jnp.bfloat16)
    att_weight, conv_weight = (
        lax.all_gather(w_out_att, "sp", axis=1, tiled=True),
        lax.all_gather(w_out_conv, "sp", axis=1, tiled=True),
    )
    terms = jnp.dot(attended, att_weight, preferred_element_type=jnp.float32) + jnp.dot(
        conv_act, conv_weight, preferred_element_type=jnp.float32
    )
    return lax.psum_scatter(terms.astype(jnp.bfloat16), "tp", scatter_dimension=1, tiled=True)


F32 = jnp.float32
BF16 = jnp.bfloat16

AT_ONCE = 1
SPLIT_FROM = 2
FAR = ((0, 1, 1, 5), (0, 2, 3, 3), (0, 0, 0, 0), (0, 0, 0, 0))
NEAR = (0, 0, 0, 0)
PASS = ((2, 2, 3, 3), (2, 3, 4, 4), (2, 4, 6, 6), (2, 3, 6, 7))


def fused_kernel(
    n_sp,
    n_tp,
    tokens_h,
    gain_h,
    wq_h,
    wk_h,
    wv_h,
    wcv_h,
    wcg_h,
    taps_h,
    cgain_h,
    cbias_h,
    gate_h,
    woa_h,
    woc_h,
    out_r,
    tok,
    normed,
    wq,
    wkv,
    wcv,
    wcg,
    taps,
    gate,
    gain_v,
    cgain_v,
    cbias_v,
    wbuf,
    kv,
    query,
    pad,
    rim_out,
    rim_in,
    stat,
    act,
    acc,
    pair_out,
    pair_in,
    sum_out,
    sum_in,
    local_sem,
    tok_send,
    tok_recv,
    w_send,
    w_recv,
    kv_send,
    kv_recv,
    rim_sem,
    stat_send,
    stat_recv,
    act_send,
    act_recv,
    pair_send,
    pair_recv,
    sum_send,
    sum_recv,
):
    scope = jax.named_scope
    s = lax.axis_index("sp")
    t = lax.axis_index("tp")
    rem = lax.rem
    last = n_sp // 2 - 1
    core = t + 1 - 2 * rem(t, 2)
    cross = rem(t + 2, n_tp)
    diag = rem(core + 2, n_tp)
    y = rem(s, 2)
    z = s // 2
    side = s + 1 - 2 * y
    mate = (z + 1 - 2 * rem(z, 2)) * 2 + y
    far = (last - z) * 2 + y
    after = rem(s + 1, n_sp)
    up = rem(s + 2, n_sp)
    up_two = rem(s + 4, n_sp)
    home = (t == z) | (t == last - z)
    near_mine = rem(t, 2) == rem(z, 2)

    rows_in = tokens_h.shape[0]
    rows = rows_in * n_tp
    head_count = gate_h.shape[0]
    ccols = wcv_h.shape[1]
    half = woa_h.shape[0]
    wide = wbuf.shape[2]
    pieces = w_recv.shape[1]
    deep = wbuf.shape[1] // pieces

    def local(src, dst, index):
        copy = pltpu.make_async_copy(src, dst, local_sem.at[index])
        copy.start()
        return copy

    def remote(src, dst, send, recv, where):
        return pltpu.make_async_remote_copy(
            src_ref=src,
            dst_ref=dst,
            send_sem=send,
            recv_sem=recv,
            device_id=where,
            device_id_type=pl.DeviceIdType.MESH,
        )

    own_tok = local(tokens_h, tok.at[t], 0)
    own_a = local(woa_h, wbuf.at[y, pl.ds(0, half)], 1)
    own_b = local(woc_h, wbuf.at[y, pl.ds(half, half)], 2)
    load_gate = local(gate_h, gate, 3)
    load_gain = local(gain_h, gain_v, 10)
    kv_cols = wk_h.shape[1]
    load_k = local(wk_h, wkv.at[:, pl.ds(0, kv_cols)], 4)
    load_v = local(wv_h, wkv.at[:, pl.ds(kv_cols, kv_cols)], 5)
    load_cv = local(wcv_h, wcv, 6)
    load_cg = local(wcg_h, wcg, 7)
    load_q = local(wq_h, wq, 8)
    load_taps = local(taps_h, taps, 9)
    load_cgain = local(cgain_h, cgain_v, 11)
    load_cbias = local(cbias_h, cbias_v, 12)

    with scope("barrier"):
        barrier = pltpu.get_barrier_semaphore()
        greeted = [{"tp": core}, {"tp": cross}, {"tp": diag}, {"sp": mate, "tp": cross}]
        greeted += [{"sp": rem(s + by, n_sp)} for by in range(1, n_sp)]
        for peer in greeted:
            pl.semaphore_signal(
                barrier, inc=1, device_id=peer, device_id_type=pl.DeviceIdType.MESH
            )
        own_tok.wait()
        pl.semaphore_wait(barrier, len(greeted))

    sent = []

    def go(copy, when=None):
        if when is None:
            copy.start()
        else:
            pl.when(when)(copy.start)
        sent.append((copy, when))

    tok_half = rows_in // 2

    def tok_copy(slot, part, number, where):
        piece = tok.at[slot, pl.ds(part * tok_half, tok_half)]
        return remote(piece, piece, tok_send.at[number], tok_recv.at[slot, part], where)

    for part in range(2):
        go(tok_copy(t, part, 2 + part, {"tp": core}))
    for part in range(2):
        go(tok_copy(t, part, part, {"tp": cross}))

    def w_copy(source, target, piece, number, where):
        span = pl.ds(piece * deep, deep)
        return remote(
            wbuf.at[source, span],
            wbuf.at[target, span],
            w_send.at[number],
            w_recv.at[target, piece],
            where,
        )

    far_copies = [w_copy(y, 2 + y, piece, piece, {"sp": far}) for piece in range(pieces)]
    pass_copies = [
        w_copy(2 + y, 2 + y, piece, 2 * pieces + piece, {"sp": side}) for piece in range(pieces)
    ]

    def pass_on(layer, point):
        for copy, turn in zip(pass_copies, PASS[layer]):
            if turn == point:
                copy.wait_recv()
                copy.start()

    def w_pass(point):
        for layer in range(last + 1):
            if point in PASS[layer]:
                pl.when(z == layer)(functools.partial(pass_on, layer, point))

    def w_wait(block):
        for piece in range(pieces):
            w_copy(2 * block + 1 - y, 2 * block + 1 - y, piece, 0, {"sp": side}).wait_recv()

    own_a.wait()
    own_b.wait()
    def release(point):
        for piece in range(pieces):
            for layer in range(last + 1):
                if FAR[layer][piece] == point:
                    pl.when(z == layer)(far_copies[piece].start)
            if NEAR[piece] == point:
                go(w_copy(y, y, piece, pieces + piece, {"sp": side}))

    release(0)

    @pl.when(y == 0)
    def _():
        kv[:, pl.ds(pl.multiple_of(side * rows, rows), rows), :] = jnp.zeros(
            (2, rows, kv.shape[2]), BF16
        )

    diagonal = lax.broadcasted_iota(jnp.int32, (rows, rows), 0) == lax.broadcasted_iota(
        jnp.int32, (rows, rows), 1
    )

    def to_lanes(column):
        return jnp.sum(jnp.where(diagonal, column, 0.0), axis=0, keepdims=True)

    def to_sublanes(row):
        return jnp.sum(jnp.where(diagonal, row, 0.0), axis=1, keepdims=True)

    load_gain.wait()
    gain = gain_v[...].astype(F32)[None, :]

    def norm_rows(slot):
        floats = tok[slot].astype(F32)
        scaled = floats * lax.rsqrt(jnp.mean(floats * floats, axis=-1, keepdims=True) + 1e-06)
        normed[pl.ds(pl.multiple_of(slot * rows_in, rows_in), rows_in), :] = (
            scaled * gain
        ).astype(BF16)

    def tok_wait(slot):
        for part in range(2):
            tok_copy(slot, part, 0, {"tp": core}).wait_recv()

    mid = rows // 2
    starts = [rem(t // 2 + part, 2) * mid for part in range(2)]

    def half_rows(part, offset=0):
        return pl.ds(pl.multiple_of(offset + starts[part], mid), mid)

    def project(weight, part):
        return jnp.dot(normed[half_rows(part), :], weight[...], preferred_element_type=F32)

    own_rows = pl.ds(pl.multiple_of(s * rows, rows), rows)

    def kv_copy(slot, part, number, where):
        piece = kv.at[:, half_rows(part, slot * rows)]
        return remote(piece, piece, kv_send.at[number], kv_recv.at[slot, part], {"sp": where})

    def kv_wait(slot, part, when):
        pl.when(when)(kv_copy(slot, part, 0, side).wait_recv)

    def kv_pass(distance, part, when):
        slot = rem(s + n_sp - 2 * distance, n_sp)
        number = 2 + 4 * distance + 2 * part
        kv_wait(slot, part, when)
        if distance < last:
            go(kv_copy(slot, part, number, up), when & (z == last - 1))
        go(kv_copy(slot, part, number + 1, side), when)

    def kv_own(part):
        both = project(wkv, part).astype(BF16)
        for column in range(2):
            kv[column, half_rows(part, s * rows), :] = both[
                :, column * kv_cols : (column + 1) * kv_cols
            ]
        go(kv_copy(s, part, 3 * part + 1, up_two), z == 0)
        go(kv_copy(s, part, 3 * part, up), z < last)
        go(kv_copy(s, part, 3 * part + 2, side), y == 0)

    rim = rim_out.shape[0]

    def glu_own(part):
        glu = project(wcv, part) * jax.nn.sigmoid(project(wcg, part))
        span = pl.ds(pl.multiple_of(rim + starts[part], rim), mid)
        pad[span, :] = glu.astype(BF16).astype(F32)

    def query_own(part):
        query[half_rows(part), :] = project(wq, part).astype(BF16)

    with scope("norm0"):
        norm_rows(t)
    with scope("tokw1"):
        tok_wait(core)
    with scope("norm1"):
        norm_rows(core)
    with scope("kv0"):
        load_k.wait()
        load_v.wait()
        kv_own(0)
    release(1)
    with scope("glu0"):
        load_cv.wait()
        load_cg.wait()
        glu_own(0)
    with scope("q0"):
        load_q.wait()
        query_own(0)
    with scope("tokw2"):
        for part in range(2):
            tok_copy(cross, part, 0, {"tp": core}).wait_recv()
            go(tok_copy(cross, part, 4 + part, {"tp": core}))
    with scope("norm2"):
        norm_rows(cross)
    with scope("tokw3"):
        tok_wait(diag)
    with scope("norm3"):
        norm_rows(diag)
    with scope("kv1"):
        kv_own(1)
    with scope("glu1"):
        glu_own(1)
        rim_out[...] = pad[pl.ds(rows, rim), :].astype(BF16)
    rim_copy = remote(rim_out, rim_in, rim_sem.at[0], rim_sem.at[1], {"sp": after})
    go(rim_copy)
    with scope("q1"):
        query_own(1)
    release(2)
    w_pass(2)
    with scope("kvp1"):
        for part in range(2):
            kv_pass(1, part, z >= 1)
        for part in range(2):
            kv_pass(2, part, z == last - 1)
    release(3)
    w_pass(3)
    with scope("rimw"):
        load_taps.wait()
        rim_copy.wait_recv()
    with scope("conv"):
        pad[pl.ds(0, rim), :] = jnp.where(s == 0, 0.0, rim_in[...].astype(F32))
        lead = rim - (KW - 1)
        conv = jnp.zeros((rows, ccols), F32)
        for tap in range(KW):
            conv = conv + taps[pl.ds(tap, 1), :].astype(F32) * pad[pl.ds(lead + tap, rows), :]
        stat[t] = jnp.zeros(stat.shape[1:], F32)
        stat[t, pl.ds(0, 1), :] = to_lanes(jnp.sum(conv, axis=1, keepdims=True))
        stat[t, pl.ds(1, 1), :] = to_lanes(jnp.sum(conv * conv, axis=1, keepdims=True))

    def stat_copy(slot, number, where):
        return remote(stat.at[slot], stat.at[slot], stat_send.at[number], stat_recv.at[slot], where)

    for number, peer in enumerate((core, cross, diag)):
        go(stat_copy(t, number, {"tp": peer}))
    release(4)
    with scope("kvp2"):
        for part in range(2):
            kv_pass(2, part, z == last)
        for part in range(2):
            kv_pass(3, part, z == last)
    with scope("wp0"):
        w_pass(4)
    def act_copy(first, size, number):
        span = pl.ds(first, size)
        return remote(
            act.at[0, :, span],
            act.at[1, :, span],
            act_send.at[number],
            act_recv.at[number],
            {"sp": mate},
        )

    act_copies = [act_copy(half, ccols, 0)]
    act_copies += [act_copy(head * HEAD, HEAD, 1 + head) for head in range(head_count)]

    scale = 1.0 / math.sqrt(HEAD)

    def fold(first, past, states):
        span = pl.ds(first, past - first)
        spots = (rows, past - first)
        key_places = first + lax.broadcasted_iota(jnp.int32, spots, 1)
        allowed = key_places <= s * rows + lax.broadcasted_iota(jnp.int32, spots, 0)
        asked = jnp.concatenate(
            [query[:, head * HEAD : (head + 1) * HEAD] for head in range(head_count)], axis=0
        )
        scores = lax.dot_general(
            asked, kv[0, span], (((1,), (1,)), ((), ())), preferred_element_type=F32
        )
        tops, denoms, parts = [], [], []
        for head in range(head_count):
            query_gate = to_sublanes(gate[pl.ds(head, 1), own_rows])
            logits = (
                scores[head * rows : (head + 1) * rows] * scale
                + query_gate
                - gate[pl.ds(head, 1), span]
            )
            logits = jnp.where(allowed, logits, -1e30)
            top = jnp.max(logits, axis=-1, keepdims=True)
            if states is not None:
                top = jnp.maximum(top, states[head][0])
            weights = jnp.exp(logits - top)
            tops.append(top)
            denoms.append(jnp.sum(weights, axis=-1, keepdims=True))
            parts.append(weights.astype(BF16))
        product = jnp.dot(
            jnp.concatenate(parts, axis=0), kv[1, span], preferred_element_type=F32
        )
        result = []
        for head in range(head_count):
            denom, numer = denoms[head], product[head * rows : (head + 1) * rows]
            if states is not None:
                factor = jnp.exp(states[head][0] - tops[head])
                denom = denom + states[head][1] * factor
                numer = numer + states[head][2] * factor
            result.append((tops[head], denom, numer))
        return result

    def attend(layer):
        def arrive(distance):
            for part in range(2):
                slot = rem(side + n_sp - 2 * distance, n_sp)
                kv_wait(slot, part, True if distance else y == 1)

        block = 2 * rows
        split = layer >= SPLIT_FROM
        for distance in range(layer + 1 - split):
            arrive(distance)
        load_gate.wait()
        states = fold(block * split, (layer + 1) * block, None)
        with scope("wpx"):
            pass_on(layer, 6)
        if split:
            arrive(layer)
            states = fold(0, block, states)
        for head in range(head_count):
            unused, denom, numer = states[head]
            act[0, :, pl.ds(head * HEAD, HEAD)] = (numer / denom).astype(BF16)
            act_copies[1 + head].start()

    for layer in range(AT_ONCE):

        @pl.when(z == layer)
        def _():
            with scope("attn_early"):
                attend(layer)

    release(5)
    with scope("statw"):
        load_cgain.wait()
        load_cbias.wait()
        for peer in (core, cross, diag):
            stat_copy(peer, 0, {"tp": core}).wait_recv()

    with scope("convact"):
        totals = stat[0]
        for peer in range(1, n_tp):
            totals = totals + stat[peer]
        channels = n_tp * ccols
        mean_c = to_sublanes(totals[0:1]) / channels
        var_c = to_sublanes(totals[1:2]) / channels - mean_c * mean_c
        shaped = (conv - mean_c) * lax.rsqrt(var_c + 1e-05) * cgain_v[...].astype(F32)[
            None, :
        ] + cbias_v[...].astype(F32)[None, :]
        act[0, :, pl.ds(half, ccols)] = (shaped / (1.0 + jnp.exp(-shaped))).astype(BF16)
    go(act_copies[0])
    for layer in range(AT_ONCE, last + 1):

        @pl.when(z == layer)
        def _():
            with scope("attn_late"):
                attend(layer)

    sent.extend((copy, None) for copy in act_copies[1:] + far_copies + pass_copies)
    with scope("wp1"):
        w_pass(7)
    with scope("wnear"):
        w_wait(0)

    def columns(part):
        return pl.ds(part * wide, wide)

    def product(row_set, block, part):
        return jnp.dot(
            act[row_set], wbuf[2 * block + part], preferred_element_type=F32
        )

    def pair_copy(row_set, part):
        return remote(
            pair_out.at[row_set, :, columns(part)],
            pair_in.at[row_set, :, columns(part)],
            pair_send.at[row_set, part],
            pair_recv.at[row_set, part],
            {"tp": core},
        )

    def ship(row_set, block):
        for part in range(2):
            pair_out[row_set, :, columns(part)] = product(row_set, block, part).astype(BF16)
            pair_copy(row_set, part).start()

    def keep(row_set, block):
        for part in range(2):
            acc[row_set, :, columns(part)] = product(row_set, block, part)

    def sum_copy(source, target, part, where):
        return remote(
            sum_out.at[source, :, columns(part)],
            sum_in.at[target, :, columns(part)],
            sum_send.at[source, part],
            sum_recv.at[target, part],
            where,
        )

    away = jnp.logical_not(home)
    own_sum = [sum_copy(0, 0, part, {"tp": cross}) for part in range(2)]
    mate_home = [sum_copy(1, 1, part, {"sp": mate}) for part in range(2)]
    mate_away = [sum_copy(1, 0, part, {"sp": mate, "tp": cross}) for part in range(2)]

    def finish(row_set):
        for part in range(2):
            pair_copy(row_set, part).wait_recv()
            total = acc[row_set, :, columns(part)] + pair_in[row_set, :, columns(part)].astype(F32)
            if row_set == 0:
                acc[0, :, columns(part)] = total
            sum_out[row_set, :, columns(part)] = total.astype(BF16)
            if row_set == 0:
                pl.when(away)(own_sum[part].start)
            else:
                pl.when(home)(mate_home[part].start)
                pl.when(away)(mate_away[part].start)

    def mate_wait():
        for copy in act_copies:
            copy.wait_recv()

    def sums(mine, odd):
        with scope("a_near0"):
            if odd:
                mate_wait()
            for row_set in (1, 0) if odd else (0,):
                (keep if mine else ship)(row_set, 0)
        with scope("a_wfar"):
            w_wait(1)
        distant = ship if mine else keep
        if odd:
            with scope("a_mate"):
                distant(1, 1)
            if mine:
                distant(0, 1)
            with scope("a_fin1"):
                finish(1)
            if not mine:
                distant(0, 1)
            with scope("a_fin0"):
                finish(0)
        else:
            distant(0, 1)
            with scope("a_fin0"):
                finish(0)
            with scope("a_mate"):
                mate_wait()
            if mine:
                ship(1, 1)
                keep(1, 0)
            else:
                ship(1, 0)
                keep(1, 1)
            with scope("a_fin1"):
                finish(1)

    for odd in range(2):
        for mine in range(2):
            pl.when((rem(z, 2) == odd) & (near_mine if mine else jnp.logical_not(near_mine)))(
                functools.partial(sums, mine, odd)
            )

    @pl.when(home)
    def _():
        for part in range(2):
            with scope("c_home"):
                own_sum[part].wait_recv()
            span = columns(part)
            out_r[:, span] = (acc[0, :, span] + sum_in[0, :, span].astype(F32)).astype(BF16)

    @pl.when(away)
    def _():
        for part in range(2):
            with scope("c_away"):
                mate_home[part].wait_recv()
                mate_away[part].wait_recv()
            span = columns(part)
            out_r[:, span] = (
                sum_in[0, :, span].astype(F32) + sum_in[1, :, span].astype(F32)
            ).astype(BF16)

    for part in range(2):
        sent.extend((pair_copy(row_set, part), None) for row_set in range(2))
        sent.append((own_sum[part], away))
        sent.append((mate_home[part], None))
    with scope("sendw"):
        for copy, when in sent:
            if when is None:
                copy.wait_send()
            else:
                pl.when(when)(copy.wait_send)


def fused(n_sp, n_tp, *args):
    tokens, gain, wq, wk, wv, wcv, wcg, taps, cgain, cbias, gate, woa, woc = args
    rows_in, width = tokens.shape
    rows = rows_in * n_tp
    rim = -(-(KW - 1) // 16) * 16
    wide = woa.shape[1]
    out_wide = wide * n_sp // n_tp
    both = woa.shape[0] + woc.shape[0]
    pieces = 4
    heads = gate.shape[1]
    hbm = pl.BlockSpec(memory_space=pltpu.HBM)
    vmem = pl.BlockSpec(memory_space=pltpu.VMEM)
    dma = pltpu.SemaphoreType.DMA
    scratch = [
        pltpu.VMEM((n_tp, rows_in, width), BF16),
        pltpu.VMEM((rows, width), BF16),
        pltpu.VMEM(wq.shape, BF16),
        pltpu.VMEM((width, wk.shape[1] + wv.shape[1]), BF16),
        *[pltpu.VMEM(w.shape, BF16) for w in (wcv, wcg, taps)],
        pltpu.VMEM(gate.shape[::-1], F32),
        pltpu.VMEM(gain.shape, BF16),
        pltpu.VMEM(cgain.shape, BF16),
        pltpu.VMEM(cbias.shape, BF16),
        pltpu.VMEM((4, both, wide), BF16),
        pltpu.VMEM((2, n_sp * rows, wk.shape[1]), BF16),
        pltpu.VMEM((rows, wq.shape[1]), BF16),
        pltpu.VMEM((rim + rows, wcv.shape[1]), F32),
        pltpu.VMEM((rim, wcv.shape[1]), BF16),
        pltpu.VMEM((rim, wcv.shape[1]), BF16),
        pltpu.VMEM((n_tp, 8, rows), F32),
        pltpu.VMEM((2, rows, both), BF16),
        pltpu.VMEM((2, rows, out_wide), F32),
        *[pltpu.VMEM((2, rows, out_wide), BF16)] * 4,
        dma((13,)),
        dma((6,)),
        dma((n_tp, 2)),
        dma((3 * pieces,)),
        dma((4, pieces)),
        dma((18,)),
        dma((n_sp, 2)),
        dma((2,)),
        dma((3,)),
        dma((n_tp,)),
        dma((1 + heads,)),
        dma((1 + heads,)),
        *[dma((2, 2))] * 4,
    ]
    result = pltpu.VMEM((rows, out_wide), BF16)
    spare = 3 * rows * out_wide
    return pl.pallas_call(
        functools.partial(fused_kernel, n_sp, n_tp),
        out_shape=result,
        in_specs=[hbm] * 13,
        out_specs=vmem,
        scratch_shapes=scratch,
        compiler_params=pltpu.CompilerParams(
            collective_id=0, has_side_effects=True, vmem_limit_bytes=67_043_328 - spare
        ),
    )(
        tokens, gain, wq, wk, wv, wcv, wcg, taps,
        cgain, cbias, gate.T, woa, woc,
    )


def layer(sizes, *args):
    n_sp, n_tp = sizes["sp"], sizes["tp"]
    tokens, wq, wk, wcv, woa, woc = (args[k] for k in (0, 2, 3, 5, 11, 12))
    fits = (
        n_sp == 8
        and n_tp == 4
        and tokens.shape[0] * n_tp == HEAD
        and wk.shape[1] == HEAD
        and woa.shape[1] % HEAD == 0
        and woa.shape == woc.shape
        and wq.shape[1] == wcv.shape[1] == woa.shape[0]
    )
    if fits:
        return fused(n_sp, n_tp, *args)
    return shards(*args)


def solution(mesh):
    return jax.shard_map(
        functools.partial(layer, dict(mesh.shape)),
        mesh=mesh,
        in_specs=(
            P(("sp", "tp"), None),
            P(),
            P(None, "tp"),
            P(None, "tp"),
            P(None, "tp"),
            P(None, "tp"),
            P(None, "tp"),
            P(None, "tp"),
            P("tp"),
            P("tp"),
            P(None, "tp"),
            P("tp", "sp"),
            P("tp", "sp"),
        ),
        out_specs=P("sp", "tp"),
        check_vma=False,
    )
```

```python
import functools
import math

import jax
import jax.numpy as jnp
from jax import lax
from jax.experimental import pallas as pl
from jax.experimental.pallas import tpu as pltpu
from jax.sharding import PartitionSpec as P

HEAD = 128
CONV = 1024
KW = 31


def shifted(array, axis, by):
    peers = lax.axis_size(axis)
    pairs = [(i, i + by) for i in range(peers) if 0 <= i + by < peers]
    return lax.ppermute(array, axis, pairs)


def shards(
    tokens,
    norm_gain,
    w_query,
    w_key,
    w_value,
    w_conv_value,
    w_conv_gate,
    conv_taps,
    conv_gain,
    conv_bias,
    cum_gate,
    w_out_att,
    w_out_conv,
):
    query_cols = w_query.shape[1]
    kv_cols = w_key.shape[1]
    conv_cols = w_conv_value.shape[1]
    head_count = query_cols // HEAD
    kv_count = kv_cols // HEAD
    group_size = head_count // kv_count
    gain_float = norm_gain.astype(jnp.float32)
    floats = lax.all_gather(tokens, "tp", axis=0, tiled=True).astype(jnp.float32)
    normed = (
        floats * lax.rsqrt(jnp.mean(floats * floats, axis=-1, keepdims=True) + 1e-06) * gain_float
    ).astype(jnp.bfloat16)
    query_part = jnp.dot(normed, w_query, preferred_element_type=jnp.float32).astype(jnp.bfloat16)
    key_part = jnp.dot(normed, w_key, preferred_element_type=jnp.float32).astype(jnp.bfloat16)
    value_part = jnp.dot(normed, w_value, preferred_element_type=jnp.float32).astype(jnp.bfloat16)
    value_glu = jnp.dot(normed, w_conv_value, preferred_element_type=jnp.float32)
    gate_glu = jnp.dot(normed, w_conv_gate, preferred_element_type=jnp.float32)
    glu_part = (value_glu * jax.nn.sigmoid(gate_glu)).astype(jnp.bfloat16)
    joined = jnp.concatenate([query_part, key_part, value_part, glu_part], axis=1)
    local_rows = joined.shape[0]
    query = joined[:, :query_cols]
    key_rows = joined[:, query_cols : query_cols + kv_cols]
    value_rows = joined[:, query_cols + kv_cols : query_cols + 2 * kv_cols]
    glu = joined[:, query_cols + 2 * kv_cols :]
    offset = lax.axis_index("sp") * local_rows
    query_places = offset + jnp.arange(local_rows, dtype=jnp.int32)
    query_gate = lax.dynamic_slice_in_dim(cum_gate, offset, local_rows, 0).T
    query_groups = query.reshape(local_rows, kv_count, group_size, HEAD)
    scale = 1.0 / math.sqrt(HEAD)

    def attend_block(state, key_block, value_block, key_start):
        run_max, run_sum, run_acc = state
        span = key_block.shape[0]
        key_heads = key_block.reshape(span, kv_count, HEAD)
        value_heads = value_block.reshape(span, kv_count, HEAD)
        scores = (
            jnp.einsum(
                "tkgd,skd->kgts", query_groups, key_heads, preferred_element_type=jnp.float32
            ).reshape(head_count, local_rows, span)
            * scale
        )
        key_gate = lax.dynamic_slice_in_dim(cum_gate, key_start, span, 0).T
        logits = scores + query_gate[:, :, None] - key_gate[:, None, :]
        key_places = key_start + jnp.arange(span, dtype=jnp.int32)
        allowed = (key_places[None, :] <= query_places[:, None])[None]
        logits = jnp.where(allowed, logits, -1e30)
        new_max = jnp.maximum(run_max, jnp.max(logits, axis=-1))
        weights = jnp.where(allowed, jnp.exp(logits - new_max[:, :, None]), 0.0)
        factor = jnp.exp(run_max - new_max)
        new_sum = run_sum * factor + jnp.sum(weights, axis=-1)
        grouped = weights.astype(jnp.bfloat16).reshape(kv_count, group_size, local_rows, span)
        product = jnp.einsum(
            "kgts,skd->kgtd", grouped, value_heads, preferred_element_type=jnp.float32
        ).reshape(head_count, local_rows, HEAD)
        new_acc = run_acc * factor[:, :, None] + product
        return (new_max, new_sum, new_acc)

    shard_rows = key_rows.shape[0]

    def fold_keys(state, pieces, start):
        key_piece, value_piece = pieces
        span = key_piece.shape[0]
        shards_in = span // shard_rows
        group = 1
        for divisor in range(1, shards_in + 1):
            if shards_in % divisor == 0 and divisor * shard_rows <= 2048:
                group = divisor
        block = group * shard_rows
        if block >= span:
            return attend_block(state, key_piece, value_piece, start)
        key_blocks = key_piece.reshape(span // block, block, kv_cols)
        value_blocks = value_piece.reshape(span // block, block, kv_cols)
        firsts = start + block * jnp.arange(span // block, dtype=jnp.int32)

        def step_block(inner, items):
            return (attend_block(inner, items[0], items[1], items[2]), None)

        result, unused = lax.scan(step_block, state, (key_blocks, value_blocks, firsts))
        return result

    start_state = (
        jnp.full((head_count, local_rows), -1e30, jnp.float32),
        jnp.zeros((head_count, local_rows), jnp.float32),
        jnp.zeros((head_count, local_rows, HEAD), jnp.float32),
    )
    run_max, run_sum, run_acc = fold_keys(
        start_state,
        (
            lax.all_gather(key_rows, "sp", axis=0, tiled=True),
            lax.all_gather(value_rows, "sp", axis=0, tiled=True),
        ),
        jnp.int32(0),
    )
    attended = jnp.transpose(
        (run_acc / run_sum[:, :, None]).astype(jnp.bfloat16), (1, 0, 2)
    ).reshape(local_rows, query_cols)
    rim = shifted(glu[local_rows - (KW - 1) :], "sp", 1)
    padded = jnp.concatenate([rim, glu], axis=0).astype(jnp.float32)
    taps = conv_taps.astype(jnp.float32)
    conv = jnp.zeros((local_rows, conv_cols), jnp.float32)
    for shift_tap in range(KW):
        conv = conv + taps[shift_tap][None, :] * padded[shift_tap : shift_tap + local_rows]
    first_sum, square_sum = lax.psum((jnp.sum(conv, axis=1), jnp.sum(conv * conv, axis=1)), "tp")
    mean_c = (first_sum / CONV)[:, None]
    var_c = (square_sum / CONV)[:, None] - mean_c * mean_c
    shaped = (conv - mean_c) * lax.rsqrt(var_c + 1e-05) * conv_gain.astype(
        jnp.float32
    ) + conv_bias.astype(jnp.float32)
    conv_act = jax.nn.silu(shaped).astype(jnp.bfloat16)
    att_weight, conv_weight = (
        lax.all_gather(w_out_att, "sp", axis=1, tiled=True),
        lax.all_gather(w_out_conv, "sp", axis=1, tiled=True),
    )
    terms = jnp.dot(attended, att_weight, preferred_element_type=jnp.float32) + jnp.dot(
        conv_act, conv_weight, preferred_element_type=jnp.float32
    )
    return lax.psum_scatter(terms.astype(jnp.bfloat16), "tp", scatter_dimension=1, tiled=True)


F32 = jnp.float32
BF16 = jnp.bfloat16

AT_ONCE = 1
SPLIT_FROM = 2
FAR = ((0, 1, 2, 5), (0, 2, 3, 3), (0, 0, 0, 0), (0, 0, 0, 0))
NEAR = (0, 0, 0, 0)
PASS = ((2, 2, 3, 3), (2, 3, 4, 4), (2, 4, 6, 6), (2, 3, 6, 7))


def fused_kernel(
    n_sp,
    n_tp,
    tokens_h,
    gain_h,
    wq_h,
    wk_h,
    wv_h,
    wcv_h,
    wcg_h,
    taps_h,
    cgain_h,
    cbias_h,
    gate_h,
    woa_h,
    woc_h,
    out_r,
    tok,
    normed,
    wq,
    wkv,
    wcv,
    wcg,
    taps,
    gate,
    gain_v,
    cgain_v,
    cbias_v,
    wbuf,
    kv,
    query,
    pad,
    rim_out,
    rim_in,
    stat,
    act,
    acc,
    pair_out,
    pair_in,
    sum_out,
    sum_in,
    local_sem,
    tok_send,
    tok_recv,
    w_send,
    w_recv,
    kv_send,
    kv_recv,
    rim_sem,
    stat_send,
    stat_recv,
    act_send,
    act_recv,
    pair_send,
    pair_recv,
    sum_send,
    sum_recv,
):
    scope = jax.named_scope
    s = lax.axis_index("sp")
    t = lax.axis_index("tp")
    rem = lax.rem
    last = n_sp // 2 - 1
    core = t + 1 - 2 * rem(t, 2)
    cross = rem(t + 2, n_tp)
    diag = rem(core + 2, n_tp)
    y = rem(s, 2)
    z = s // 2
    side = s + 1 - 2 * y
    mate = (z + 1 - 2 * rem(z, 2)) * 2 + y
    far = (last - z) * 2 + y
    after = rem(s + 1, n_sp)
    up = rem(s + 2, n_sp)
    up_two = rem(s + 4, n_sp)
    home = (t == z) | (t == last - z)
    near_mine = rem(t, 2) == rem(z, 2)

    rows_in = tokens_h.shape[0]
    rows = rows_in * n_tp
    head_count = gate_h.shape[0]
    ccols = wcv_h.shape[1]
    half = woa_h.shape[0]
    wide = wbuf.shape[2]
    pieces = w_recv.shape[0] - 2
    deep = wbuf.shape[1] // pieces

    def local(src, dst, index):
        copy = pltpu.make_async_copy(src, dst, local_sem.at[index])
        copy.start()
        return copy

    def remote(src, dst, send, recv, where):
        return pltpu.make_async_remote_copy(
            src_ref=src,
            dst_ref=dst,
            send_sem=send,
            recv_sem=recv,
            device_id=where,
            device_id_type=pl.DeviceIdType.MESH,
        )

    own_tok = local(tokens_h, tok.at[t], 0)
    local(woa_h, wbuf.at[y, pl.ds(0, half)], 1)
    local(woc_h, wbuf.at[y, pl.ds(half, half)], 1)
    load_gate = local(gate_h, gate, 3)
    load_gain = local(gain_h, gain_v, 2)
    kv_cols = wk_h.shape[1]
    local(wk_h, wkv.at[:, pl.ds(0, kv_cols)], 4)
    local(wv_h, wkv.at[:, pl.ds(kv_cols, kv_cols)], 4)
    load_cv = local(wcv_h, wcv, 6)
    load_cg = local(wcg_h, wcg, 7)
    load_q = local(wq_h, wq, 8)
    load_taps = local(taps_h, taps, 5)
    load_cgain = local(cgain_h, cgain_v, 9)
    load_cbias = local(cbias_h, cbias_v, 10)

    with scope("barrier"):
        barrier = pltpu.get_barrier_semaphore()
        greeted = [{"tp": core}, {"tp": cross}, {"tp": diag}, {"sp": mate, "tp": cross}]
        greeted += [{"sp": rem(s + by, n_sp)} for by in range(1, n_sp)]
        for peer in greeted:
            pl.semaphore_signal(
                barrier, inc=1, device_id=peer, device_id_type=pl.DeviceIdType.MESH
            )
        own_tok.wait()
        pl.semaphore_wait(barrier, len(greeted))

    sent = []

    def go(copy, when=None):
        if when is None:
            copy.start()
        else:
            pl.when(when)(copy.start)
        sent.append((copy, when))

    tok_half = rows_in // 2

    def all_sent(ref, sem, when=None):
        sent.append((remote(ref, ref, sem, sem, {"tp": core}), when))

    def tok_copy(slot, part, sends, lands, where):
        piece = tok.at[slot, pl.ds(part * tok_half, tok_half)]
        return remote(piece, piece, tok_send.at[sends], tok_recv.at[lands], where)

    for part in range(2):
        tok_copy(t, part, 0, 0, {"tp": core}).start()
    for part in range(2):
        tok_copy(t, part, 1, 1 + part, {"tp": cross}).start()
    for group, slot in enumerate((t, t, cross)):
        all_sent(tok.at[slot], tok_send.at[group])

    def w_copy(source, target, piece, sends, lands, where):
        span = pl.ds(piece * deep, deep)
        return remote(
            wbuf.at[source, span],
            wbuf.at[target, span],
            w_send.at[sends],
            w_recv.at[lands],
            where,
        )

    far_copies = [
        w_copy(y, 2 + y, piece, 0, 2 + piece, {"sp": far}) for piece in range(pieces)
    ]
    pass_copies = [w_copy(2 + y, 2 + y, piece, 2, 1, {"sp": side}) for piece in range(pieces)]
    for group, slot in enumerate((y, y, 2 + y)):
        all_sent(wbuf.at[slot], w_send.at[group])

    def pass_on(layer, point):
        for piece, turn in enumerate(PASS[layer]):
            if turn == point:
                far_copies[piece].wait_recv()
                pass_copies[piece].start()

    def w_pass(point):
        for layer in range(last + 1):
            if point in PASS[layer]:
                pl.when(z == layer)(functools.partial(pass_on, layer, point))

    def w_wait(block):
        ref = wbuf.at[2 * block + 1 - y]
        remote(ref, ref, w_send.at[0], w_recv.at[block], {"sp": side}).wait_recv()

    pltpu.make_async_copy(wbuf.at[y], wbuf.at[y], local_sem.at[1]).wait()
    def release(point):
        for piece in range(pieces):
            for layer in range(last + 1):
                if FAR[layer][piece] == point:
                    pl.when(z == layer)(far_copies[piece].start)
            if NEAR[piece] == point:
                w_copy(y, y, piece, 1, 0, {"sp": side}).start()

    release(0)

    @pl.when(y == 0)
    def _():
        kv[:, pl.ds(pl.multiple_of(side * rows, rows), rows), :] = jnp.zeros(
            (2, rows, kv.shape[2]), BF16
        )

    diagonal = lax.broadcasted_iota(jnp.int32, (rows, rows), 0) == lax.broadcasted_iota(
        jnp.int32, (rows, rows), 1
    )

    def to_lanes(column):
        return jnp.sum(jnp.where(diagonal, column, 0.0), axis=0, keepdims=True)

    def to_sublanes(row):
        return jnp.sum(jnp.where(diagonal, row, 0.0), axis=1, keepdims=True)

    load_gain.wait()
    gain = gain_v[...].astype(F32)[None, :]

    def norm_rows(slot):
        floats = tok[slot].astype(F32)
        scaled = floats * lax.rsqrt(jnp.mean(floats * floats, axis=-1, keepdims=True) + 1e-06)
        normed[pl.ds(pl.multiple_of(slot * rows_in, rows_in), rows_in), :] = (
            scaled * gain
        ).astype(BF16)

    def tok_wait(slot, lands):
        ref = tok.at[slot]
        remote(ref, ref, tok_send.at[0], tok_recv.at[lands], {"tp": core}).wait_recv()

    mid = rows // 2
    starts = [rem(t // 2 + part, 2) * mid for part in range(2)]

    def half_rows(part, offset=0):
        return pl.ds(pl.multiple_of(offset + starts[part], mid), mid)

    def project(weight, part):
        return jnp.dot(normed[half_rows(part), :], weight[...], preferred_element_type=F32)

    own_rows = pl.ds(pl.multiple_of(s * rows, rows), rows)

    def kv_copy(slot, part, sends, where):
        piece = kv.at[:, half_rows(part, slot * rows)]
        lands = n_sp + slot // 2 if where is side else 2 * (slot // 2) + part
        return remote(piece, piece, kv_send.at[sends], kv_recv.at[lands], {"sp": where})

    def kv_slot(slot):
        return kv.at[:, pl.ds(pl.multiple_of(slot * rows, rows), rows)]

    def kv_start(slot, part, sends, where, when):
        pl.when(when)(kv_copy(slot, part, sends, where).start)
        if part == 1:
            all_sent(kv_slot(slot), kv_send.at[sends], when)

    def kv_pass(distance, part, when):
        slot = rem(s + n_sp - 2 * distance, n_sp)
        pl.when(when)(kv_copy(slot, part, 0, up).wait_recv)
        if distance < last:
            kv_start(slot, part, 1 + 2 * distance, up, when & (z == last - 1))
        kv_start(slot, part, 2 + 2 * distance if distance < last else 7, side, when)

    def kv_own(part):
        both = project(wkv, part).astype(BF16)
        for column in range(2):
            kv[column, half_rows(part, s * rows), :] = both[
                :, column * kv_cols : (column + 1) * kv_cols
            ]
        kv_start(s, part, 1, up_two, z == 0)
        kv_start(s, part, 0, up, z < last)
        kv_start(s, part, 2, side, y == 0)

    rim = rim_out.shape[0]

    def glu_own(part):
        glu = project(wcv, part) * jax.nn.sigmoid(project(wcg, part))
        span = pl.ds(pl.multiple_of(rim + starts[part], rim), mid)
        pad[span, :] = glu.astype(BF16).astype(F32)

    def query_own(part):
        query[half_rows(part), :] = project(wq, part).astype(BF16)

    with scope("norm0"):
        norm_rows(t)
    with scope("tokw1"):
        tok_wait(core, 0)
    with scope("norm1"):
        norm_rows(core)
    with scope("kv0"):
        pltpu.make_async_copy(wkv, wkv, local_sem.at[4]).wait()
        kv_own(0)
    release(1)
    with scope("glu0"):
        load_cv.wait()
        load_cg.wait()
        glu_own(0)
    with scope("q0"):
        load_q.wait()
        query_own(0)
    with scope("tokw2"):
        for part in range(2):
            tok_copy(cross, part, 1, 1 + part, {"tp": cross}).wait_recv()
            tok_copy(cross, part, 2, 3, {"tp": core}).start()
    with scope("norm2"):
        norm_rows(cross)
    with scope("tokw3"):
        tok_wait(diag, 3)
    with scope("norm3"):
        norm_rows(diag)
    with scope("kv1"):
        kv_own(1)
    with scope("glu1"):
        glu_own(1)
        rim_out[...] = pad[pl.ds(rows, rim), :].astype(BF16)
    rim_copy = remote(rim_out, rim_in, rim_sem.at[0], rim_sem.at[1], {"sp": after})
    go(rim_copy)
    with scope("q1"):
        query_own(1)
    release(2)
    w_pass(2)
    with scope("kvp1"):
        for part in range(2):
            kv_pass(1, part, z >= 1)
        for part in range(2):
            kv_pass(2, part, z == last - 1)
    release(3)
    w_pass(3)
    with scope("rimw"):
        load_taps.wait()
        rim_copy.wait_recv()
    with scope("conv"):
        pad[pl.ds(0, rim), :] = jnp.where(s == 0, 0.0, rim_in[...].astype(F32))
        lead = rim - (KW - 1)
        conv = jnp.zeros((rows, ccols), F32)
        for tap in range(KW):
            conv = conv + taps[pl.ds(tap, 1), :].astype(F32) * pad[pl.ds(lead + tap, rows), :]
        stat[t] = jnp.zeros(stat.shape[1:], F32)
        stat[t, pl.ds(0, 1), :] = to_lanes(jnp.sum(conv, axis=1, keepdims=True))
        stat[t, pl.ds(1, 1), :] = to_lanes(jnp.sum(conv * conv, axis=1, keepdims=True))

    others = stat.at[pl.ds(0, n_tp - 1)]
    for peer in (core, cross, diag):
        remote(
            stat.at[t], stat.at[t], stat_send.at[0], stat_recv.at[0], {"tp": peer}
        ).start()
    all_sent(others, stat_send.at[0])
    release(4)
    with scope("kvp2"):
        for part in range(2):
            kv_pass(2, part, z == last)
        for part in range(2):
            kv_pass(3, part, z == last)
    with scope("wp0"):
        w_pass(4)
    def act_copy(first, size):
        span = pl.ds(first, size)
        return remote(
            act.at[0, :, span],
            act.at[1, :, span],
            act_send.at[0],
            act_recv.at[0],
            {"sp": mate},
        )

    act_copies = [act_copy(half, ccols)]
    act_copies += [act_copy(head * HEAD, HEAD) for head in range(head_count)]
    whole_act = act_copy(0, half + ccols)

    scale = 1.0 / math.sqrt(HEAD)

    def fold(first, past, states):
        span = pl.ds(first, past - first)
        spots = (rows, past - first)
        key_places = first + lax.broadcasted_iota(jnp.int32, spots, 1)
        allowed = key_places <= s * rows + lax.broadcasted_iota(jnp.int32, spots, 0)
        asked = jnp.concatenate(
            [query[:, head * HEAD : (head + 1) * HEAD] for head in range(head_count)], axis=0
        )
        scores = lax.dot_general(
            asked, kv[0, span], (((1,), (1,)), ((), ())), preferred_element_type=F32
        )
        tops, denoms, parts = [], [], []
        for head in range(head_count):
            query_gate = to_sublanes(gate[pl.ds(head, 1), own_rows])
            logits = (
                scores[head * rows : (head + 1) * rows] * scale
                + query_gate
                - gate[pl.ds(head, 1), span]
            )
            logits = jnp.where(allowed, logits, -1e30)
            top = jnp.max(logits, axis=-1, keepdims=True)
            if states is not None:
                top = jnp.maximum(top, states[head][0])
            weights = jnp.exp(logits - top)
            tops.append(top)
            denoms.append(jnp.sum(weights, axis=-1, keepdims=True))
            parts.append(weights.astype(BF16))
        product = jnp.dot(
            jnp.concatenate(parts, axis=0), kv[1, span], preferred_element_type=F32
        )
        result = []
        for head in range(head_count):
            denom, numer = denoms[head], product[head * rows : (head + 1) * rows]
            if states is not None:
                factor = jnp.exp(states[head][0] - tops[head])
                denom = denom + states[head][1] * factor
                numer = numer + states[head][2] * factor
            result.append((tops[head], denom, numer))
        return result

    def attend(layer):
        def arrive(distance):
            slot = rem(side + n_sp - 2 * distance, n_sp)
            ref = kv_slot(slot)
            copy = remote(
                ref, ref, kv_send.at[0], kv_recv.at[n_sp + slot // 2], {"sp": side}
            )
            pl.when(True if distance else y == 1)(copy.wait_recv)

        block = 2 * rows
        split = layer >= SPLIT_FROM
        for distance in range(layer + 1 - split):
            arrive(distance)
        load_gate.wait()
        states = fold(block * split, (layer + 1) * block, None)
        with scope("wpx"):
            pass_on(layer, 6)
        if split:
            arrive(layer)
            states = fold(0, block, states)
        for head in range(head_count):
            unused, denom, numer = states[head]
            act[0, :, pl.ds(head * HEAD, HEAD)] = (numer / denom).astype(BF16)
            act_copies[1 + head].start()

    for layer in range(AT_ONCE):

        @pl.when(z == layer)
        def _():
            with scope("attn_early"):
                attend(layer)

    release(5)
    with scope("statw"):
        load_cgain.wait()
        load_cbias.wait()
        remote(others, others, stat_send.at[0], stat_recv.at[0], {"tp": core}).wait_recv()

    with scope("convact"):
        totals = stat[0]
        for peer in range(1, n_tp):
            totals = totals + stat[peer]
        channels = n_tp * ccols
        mean_c = to_sublanes(totals[0:1]) / channels
        var_c = to_sublanes(totals[1:2]) / channels - mean_c * mean_c
        shaped = (conv - mean_c) * lax.rsqrt(var_c + 1e-05) * cgain_v[...].astype(F32)[
            None, :
        ] + cbias_v[...].astype(F32)[None, :]
        act[0, :, pl.ds(half, ccols)] = (shaped / (1.0 + jnp.exp(-shaped))).astype(BF16)
    act_copies[0].start()
    for layer in range(AT_ONCE, last + 1):

        @pl.when(z == layer)
        def _():
            with scope("attn_late"):
                attend(layer)

    sent.append((whole_act, None))
    with scope("wp1"):
        w_pass(7)
    with scope("wnear"):
        w_wait(0)

    def columns(part):
        return pl.ds(part * wide, wide)

    def product(row_set, block, part):
        return jnp.dot(
            act[row_set], wbuf[2 * block + part], preferred_element_type=F32
        )

    def pair_copy(row_set, part):
        return remote(
            pair_out.at[row_set, :, columns(part)],
            pair_in.at[row_set, :, columns(part)],
            pair_send.at[row_set],
            pair_recv.at[row_set, part],
            {"tp": core},
        )

    def ship(row_set, block):
        for part in range(2):
            pair_out[row_set, :, columns(part)] = product(row_set, block, part).astype(BF16)
            pair_copy(row_set, part).start()

    def keep(row_set, block):
        for part in range(2):
            acc[row_set, :, columns(part)] = product(row_set, block, part)

    def sum_copy(source, target, part, where):
        return remote(
            sum_out.at[source, :, columns(part)],
            sum_in.at[target, :, columns(part)],
            sum_send.at[source],
            sum_recv.at[target, part],
            where,
        )

    away = jnp.logical_not(home)
    own_sum = [sum_copy(0, 0, part, {"tp": cross}) for part in range(2)]
    mate_home = [sum_copy(1, 1, part, {"sp": mate}) for part in range(2)]
    mate_away = [sum_copy(1, 0, part, {"sp": mate, "tp": cross}) for part in range(2)]

    def finish(row_set):
        for part in range(2):
            pair_copy(row_set, part).wait_recv()
            total = acc[row_set, :, columns(part)] + pair_in[row_set, :, columns(part)].astype(F32)
            if row_set == 0:
                acc[0, :, columns(part)] = total
            sum_out[row_set, :, columns(part)] = total.astype(BF16)
            if row_set == 0:
                pl.when(away)(own_sum[part].start)
            else:
                pl.when(home)(mate_home[part].start)
                pl.when(away)(mate_away[part].start)

    def mate_wait():
        whole_act.wait_recv()

    def sums(mine, odd):
        with scope("a_near0"):
            if odd:
                mate_wait()
            for row_set in (1, 0) if odd else (0,):
                (keep if mine else ship)(row_set, 0)
        with scope("a_wfar"):
            w_wait(1)
        distant = ship if mine else keep
        if odd:
            with scope("a_mate"):
                distant(1, 1)
            if mine:
                distant(0, 1)
            with scope("a_fin1"):
                finish(1)
            if not mine:
                distant(0, 1)
            with scope("a_fin0"):
                finish(0)
        else:
            distant(0, 1)
            with scope("a_fin0"):
                finish(0)
            with scope("a_mate"):
                mate_wait()
            if mine:
                ship(1, 1)
                keep(1, 0)
            else:
                ship(1, 0)
                keep(1, 1)
            with scope("a_fin1"):
                finish(1)

    for odd in range(2):
        for mine in range(2):
            pl.when((rem(z, 2) == odd) & (near_mine if mine else jnp.logical_not(near_mine)))(
                functools.partial(sums, mine, odd)
            )

    @pl.when(home)
    def _():
        for part in range(2):
            with scope("c_home"):
                own_sum[part].wait_recv()
            span = columns(part)
            out_r[:, span] = (acc[0, :, span] + sum_in[0, :, span].astype(F32)).astype(BF16)

    @pl.when(away)
    def _():
        for part in range(2):
            with scope("c_away"):
                mate_home[part].wait_recv()
                mate_away[part].wait_recv()
            span = columns(part)
            out_r[:, span] = (
                sum_in[0, :, span].astype(F32) + sum_in[1, :, span].astype(F32)
            ).astype(BF16)

    for row_set in range(2):
        all_sent(pair_out.at[row_set], pair_send.at[row_set])
    all_sent(sum_out.at[0], sum_send.at[0], away)
    all_sent(sum_out.at[1], sum_send.at[1])
    with scope("sendw"):
        for copy, when in sent:
            if when is None:
                copy.wait_send()
            else:
                pl.when(when)(copy.wait_send)


def fused(n_sp, n_tp, *args):
    tokens, gain, wq, wk, wv, wcv, wcg, taps, cgain, cbias, gate, woa, woc = args
    rows_in, width = tokens.shape
    rows = rows_in * n_tp
    rim = -(-(KW - 1) // 16) * 16
    wide = woa.shape[1]
    out_wide = wide * n_sp // n_tp
    both = woa.shape[0] + woc.shape[0]
    pieces = 4
    hbm = pl.BlockSpec(memory_space=pltpu.HBM)
    vmem = pl.BlockSpec(memory_space=pltpu.VMEM)
    dma = pltpu.SemaphoreType.DMA
    scratch = [
        pltpu.VMEM((n_tp, rows_in, width), BF16),
        pltpu.VMEM((rows, width), BF16),
        pltpu.VMEM(wq.shape, BF16),
        pltpu.VMEM((width, wk.shape[1] + wv.shape[1]), BF16),
        *[pltpu.VMEM(w.shape, BF16) for w in (wcv, wcg, taps)],
        pltpu.VMEM(gate.shape[::-1], F32),
        pltpu.VMEM(gain.shape, BF16),
        pltpu.VMEM(cgain.shape, BF16),
        pltpu.VMEM(cbias.shape, BF16),
        pltpu.VMEM((4, both, wide), BF16),
        pltpu.VMEM((2, n_sp * rows, wk.shape[1]), BF16),
        pltpu.VMEM((rows, wq.shape[1]), BF16),
        pltpu.VMEM((rim + rows, wcv.shape[1]), F32),
        pltpu.VMEM((rim, wcv.shape[1]), BF16),
        pltpu.VMEM((rim, wcv.shape[1]), BF16),
        pltpu.VMEM((n_tp, 8, rows), F32),
        pltpu.VMEM((2, rows, both), BF16),
        pltpu.VMEM((2, rows, out_wide), F32),
        *[pltpu.VMEM((2, rows, out_wide), BF16)] * 4,
        dma((11,)),
        dma((3,)),
        dma((4,)),
        dma((3,)),
        dma((2 + pieces,)),
        dma((8,)),
        dma((n_sp + n_sp // 2,)),
        dma((2,)),
        *[dma((1,))] * 4,
        *[dma((2,)), dma((2, 2))] * 2,
    ]
    result = pltpu.VMEM((rows, out_wide), BF16)
    spare = 3 * rows * out_wide
    return pl.pallas_call(
        functools.partial(fused_kernel, n_sp, n_tp),
        out_shape=result,
        in_specs=[hbm] * 13,
        out_specs=vmem,
        scratch_shapes=scratch,
        compiler_params=pltpu.CompilerParams(
            collective_id=0, has_side_effects=True, vmem_limit_bytes=67_043_328 - spare
        ),
    )(
        tokens, gain, wq, wk, wv, wcv, wcg, taps,
        cgain, cbias, gate.T, woa, woc,
    )


def layer(sizes, *args):
    n_sp, n_tp = sizes["sp"], sizes["tp"]
    tokens, wq, wk, wcv, woa, woc = (args[k] for k in (0, 2, 3, 5, 11, 12))
    fits = (
        n_sp == 8
        and n_tp == 4
        and tokens.shape[0] * n_tp == HEAD
        and wk.shape[1] == HEAD
        and woa.shape[1] % HEAD == 0
        and woa.shape == woc.shape
        and wq.shape[1] == wcv.shape[1] == woa.shape[0]
    )
    if fits:
        return fused(n_sp, n_tp, *args)
    return shards(*args)


def solution(mesh):
    return jax.shard_map(
        functools.partial(layer, dict(mesh.shape)),
        mesh=mesh,
        in_specs=(
            P(("sp", "tp"), None),
            P(),
            P(None, "tp"),
            P(None, "tp"),
            P(None, "tp"),
            P(None, "tp"),
            P(None, "tp"),
            P(None, "tp"),
            P("tp"),
            P("tp"),
            P(None, "tp"),
            P("tp", "sp"),
            P("tp", "sp"),
        ),
        out_specs=P("sp", "tp"),
        check_vma=False,
    )
```

```python
import functools
import math

import jax
import jax.numpy as jnp
from jax import lax
from jax.experimental import pallas as pl
from jax.experimental.pallas import tpu as pltpu
from jax.sharding import PartitionSpec as P

HEAD = 128
CONV = 1024
KW = 31


def shifted(array, axis, by):
    peers = lax.axis_size(axis)
    pairs = [(i, i + by) for i in range(peers) if 0 <= i + by < peers]
    return lax.ppermute(array, axis, pairs)


def shards(
    tokens,
    norm_gain,
    w_query,
    w_key,
    w_value,
    w_conv_value,
    w_conv_gate,
    conv_taps,
    conv_gain,
    conv_bias,
    cum_gate,
    w_out_att,
    w_out_conv,
):
    query_cols = w_query.shape[1]
    kv_cols = w_key.shape[1]
    conv_cols = w_conv_value.shape[1]
    head_count = query_cols // HEAD
    kv_count = kv_cols // HEAD
    group_size = head_count // kv_count
    gain_float = norm_gain.astype(jnp.float32)
    floats = lax.all_gather(tokens, "tp", axis=0, tiled=True).astype(jnp.float32)
    normed = (
        floats * lax.rsqrt(jnp.mean(floats * floats, axis=-1, keepdims=True) + 1e-06) * gain_float
    ).astype(jnp.bfloat16)
    query_part = jnp.dot(normed, w_query, preferred_element_type=jnp.float32).astype(jnp.bfloat16)
    key_part = jnp.dot(normed, w_key, preferred_element_type=jnp.float32).astype(jnp.bfloat16)
    value_part = jnp.dot(normed, w_value, preferred_element_type=jnp.float32).astype(jnp.bfloat16)
    value_glu = jnp.dot(normed, w_conv_value, preferred_element_type=jnp.float32)
    gate_glu = jnp.dot(normed, w_conv_gate, preferred_element_type=jnp.float32)
    glu_part = (value_glu * jax.nn.sigmoid(gate_glu)).astype(jnp.bfloat16)
    joined = jnp.concatenate([query_part, key_part, value_part, glu_part], axis=1)
    local_rows = joined.shape[0]
    query = joined[:, :query_cols]
    key_rows = joined[:, query_cols : query_cols + kv_cols]
    value_rows = joined[:, query_cols + kv_cols : query_cols + 2 * kv_cols]
    glu = joined[:, query_cols + 2 * kv_cols :]
    offset = lax.axis_index("sp") * local_rows
    query_places = offset + jnp.arange(local_rows, dtype=jnp.int32)
    query_gate = lax.dynamic_slice_in_dim(cum_gate, offset, local_rows, 0).T
    query_groups = query.reshape(local_rows, kv_count, group_size, HEAD)
    scale = 1.0 / math.sqrt(HEAD)

    def attend_block(state, key_block, value_block, key_start):
        run_max, run_sum, run_acc = state
        span = key_block.shape[0]
        key_heads = key_block.reshape(span, kv_count, HEAD)
        value_heads = value_block.reshape(span, kv_count, HEAD)
        scores = (
            jnp.einsum(
                "tkgd,skd->kgts", query_groups, key_heads, preferred_element_type=jnp.float32
            ).reshape(head_count, local_rows, span)
            * scale
        )
        key_gate = lax.dynamic_slice_in_dim(cum_gate, key_start, span, 0).T
        logits = scores + query_gate[:, :, None] - key_gate[:, None, :]
        key_places = key_start + jnp.arange(span, dtype=jnp.int32)
        allowed = (key_places[None, :] <= query_places[:, None])[None]
        logits = jnp.where(allowed, logits, -1e30)
        new_max = jnp.maximum(run_max, jnp.max(logits, axis=-1))
        weights = jnp.where(allowed, jnp.exp(logits - new_max[:, :, None]), 0.0)
        factor = jnp.exp(run_max - new_max)
        new_sum = run_sum * factor + jnp.sum(weights, axis=-1)
        grouped = weights.astype(jnp.bfloat16).reshape(kv_count, group_size, local_rows, span)
        product = jnp.einsum(
            "kgts,skd->kgtd", grouped, value_heads, preferred_element_type=jnp.float32
        ).reshape(head_count, local_rows, HEAD)
        new_acc = run_acc * factor[:, :, None] + product
        return (new_max, new_sum, new_acc)

    shard_rows = key_rows.shape[0]

    def fold_keys(state, pieces, start):
        key_piece, value_piece = pieces
        span = key_piece.shape[0]
        shards_in = span // shard_rows
        group = 1
        for divisor in range(1, shards_in + 1):
            if shards_in % divisor == 0 and divisor * shard_rows <= 2048:
                group = divisor
        block = group * shard_rows
        if block >= span:
            return attend_block(state, key_piece, value_piece, start)
        key_blocks = key_piece.reshape(span // block, block, kv_cols)
        value_blocks = value_piece.reshape(span // block, block, kv_cols)
        firsts = start + block * jnp.arange(span // block, dtype=jnp.int32)

        def step_block(inner, items):
            return (attend_block(inner, items[0], items[1], items[2]), None)

        result, unused = lax.scan(step_block, state, (key_blocks, value_blocks, firsts))
        return result

    start_state = (
        jnp.full((head_count, local_rows), -1e30, jnp.float32),
        jnp.zeros((head_count, local_rows), jnp.float32),
        jnp.zeros((head_count, local_rows, HEAD), jnp.float32),
    )
    run_max, run_sum, run_acc = fold_keys(
        start_state,
        (
            lax.all_gather(key_rows, "sp", axis=0, tiled=True),
            lax.all_gather(value_rows, "sp", axis=0, tiled=True),
        ),
        jnp.int32(0),
    )
    attended = jnp.transpose(
        (run_acc / run_sum[:, :, None]).astype(jnp.bfloat16), (1, 0, 2)
    ).reshape(local_rows, query_cols)
    rim = shifted(glu[local_rows - (KW - 1) :], "sp", 1)
    padded = jnp.concatenate([rim, glu], axis=0).astype(jnp.float32)
    taps = conv_taps.astype(jnp.float32)
    conv = jnp.zeros((local_rows, conv_cols), jnp.float32)
    for shift_tap in range(KW):
        conv = conv + taps[shift_tap][None, :] * padded[shift_tap : shift_tap + local_rows]
    first_sum, square_sum = lax.psum((jnp.sum(conv, axis=1), jnp.sum(conv * conv, axis=1)), "tp")
    mean_c = (first_sum / CONV)[:, None]
    var_c = (square_sum / CONV)[:, None] - mean_c * mean_c
    shaped = (conv - mean_c) * lax.rsqrt(var_c + 1e-05) * conv_gain.astype(
        jnp.float32
    ) + conv_bias.astype(jnp.float32)
    conv_act = jax.nn.silu(shaped).astype(jnp.bfloat16)
    att_weight, conv_weight = (
        lax.all_gather(w_out_att, "sp", axis=1, tiled=True),
        lax.all_gather(w_out_conv, "sp", axis=1, tiled=True),
    )
    terms = jnp.dot(attended, att_weight, preferred_element_type=jnp.float32) + jnp.dot(
        conv_act, conv_weight, preferred_element_type=jnp.float32
    )
    return lax.psum_scatter(terms.astype(jnp.bfloat16), "tp", scatter_dimension=1, tiled=True)


F32 = jnp.float32
BF16 = jnp.bfloat16

AT_ONCE = 1
SPLIT_FROM = 2
FAR = ((0, 0, 1, 1, 2, 2, 5, 5), (0, 0, 2, 2, 3, 3, 3, 3), (0, 0, 0, 0, 0, 0, 0, 0), (0, 0, 0, 0, 0, 0, 0, 0))
NEAR = (0, 0, 0, 0, 0, 0, 0, 0)
PASS = ((2, 2, 2, 2, 3, 3, 3, 3), (2, 2, 3, 3, 4, 4, 4, 4), (2, 2, 4, 4, 6, 6, 6, 7), (2, 2, 3, 3, 6, 6, 7, 7))


def fused_kernel(
    n_sp,
    n_tp,
    tokens_h,
    gain_h,
    wq_h,
    wk_h,
    wv_h,
    wcv_h,
    wcg_h,
    taps_h,
    cgain_h,
    cbias_h,
    gate_h,
    woa_h,
    woc_h,
    out_r,
    tok,
    normed,
    wq,
    wkv,
    wcv,
    wcg,
    taps,
    gate,
    gain_v,
    cgain_v,
    cbias_v,
    wbuf,
    kv,
    query,
    pad,
    rim_out,
    rim_in,
    stat,
    act,
    acc,
    pair_out,
    pair_in,
    sum_out,
    sum_in,
    local_sem,
    tok_send,
    tok_recv,
    w_send,
    w_recv,
    kv_send,
    kv_recv,
    rim_sem,
    stat_send,
    stat_recv,
    act_send,
    act_recv,
    pair_send,
    pair_recv,
    sum_send,
    sum_recv,
):
    scope = jax.named_scope
    s = lax.axis_index("sp")
    t = lax.axis_index("tp")
    rem = lax.rem
    last = n_sp // 2 - 1
    core = t + 1 - 2 * rem(t, 2)
    cross = rem(t + 2, n_tp)
    diag = rem(core + 2, n_tp)
    y = rem(s, 2)
    z = s // 2
    side = s + 1 - 2 * y
    mate = (z + 1 - 2 * rem(z, 2)) * 2 + y
    far = (last - z) * 2 + y
    after = rem(s + 1, n_sp)
    up = rem(s + 2, n_sp)
    up_two = rem(s + 4, n_sp)
    home = (t == z) | (t == last - z)
    near_mine = rem(t, 2) == rem(z, 2)

    rows_in = tokens_h.shape[0]
    rows = rows_in * n_tp
    head_count = gate_h.shape[0]
    ccols = wcv_h.shape[1]
    half = woa_h.shape[0]
    wide = wbuf.shape[2]
    pieces = w_recv.shape[0] - 2
    deep = wbuf.shape[1] // pieces

    def local(src, dst, index):
        copy = pltpu.make_async_copy(src, dst, local_sem.at[index])
        copy.start()
        return copy

    def remote(src, dst, send, recv, where):
        return pltpu.make_async_remote_copy(
            src_ref=src,
            dst_ref=dst,
            send_sem=send,
            recv_sem=recv,
            device_id=where,
            device_id_type=pl.DeviceIdType.MESH,
        )

    own_tok = local(tokens_h, tok.at[t], 0)
    local(woa_h, wbuf.at[y, pl.ds(0, half)], 1)
    local(woc_h, wbuf.at[y, pl.ds(half, half)], 1)
    load_gate = local(gate_h, gate, 3)
    load_gain = local(gain_h, gain_v, 2)
    kv_cols = wk_h.shape[1]
    local(wk_h, wkv.at[:, pl.ds(0, kv_cols)], 4)
    local(wv_h, wkv.at[:, pl.ds(kv_cols, kv_cols)], 4)
    load_cv = local(wcv_h, wcv, 6)
    load_cg = local(wcg_h, wcg, 7)
    load_q = local(wq_h, wq, 8)
    load_taps = local(taps_h, taps, 5)
    load_cgain = local(cgain_h, cgain_v, 9)
    load_cbias = local(cbias_h, cbias_v, 10)

    with scope("barrier"):
        barrier = pltpu.get_barrier_semaphore()
        greeted = [{"tp": core}, {"tp": cross}, {"tp": diag}, {"sp": mate, "tp": cross}]
        greeted += [{"sp": rem(s + by, n_sp)} for by in range(1, n_sp)]
        for peer in greeted:
            pl.semaphore_signal(
                barrier, inc=1, device_id=peer, device_id_type=pl.DeviceIdType.MESH
            )
        own_tok.wait()
        pl.semaphore_wait(barrier, len(greeted))

    sent = []

    def go(copy, when=None):
        if when is None:
            copy.start()
        else:
            pl.when(when)(copy.start)
        sent.append((copy, when))

    tok_half = rows_in // 2

    def all_sent(ref, sem, when=None):
        sent.append((remote(ref, ref, sem, sem, {"tp": core}), when))

    def tok_copy(slot, part, sends, lands, where):
        piece = tok.at[slot, pl.ds(part * tok_half, tok_half)]
        return remote(piece, piece, tok_send.at[sends], tok_recv.at[lands], where)

    for part in range(2):
        tok_copy(t, part, 0, 0, {"tp": core}).start()
    for part in range(2):
        tok_copy(t, part, 1, 1 + part, {"tp": cross}).start()
    for group, slot in enumerate((t, t, cross)):
        all_sent(tok.at[slot], tok_send.at[group])

    def w_copy(source, target, piece, sends, lands, where):
        span = pl.ds(piece * deep, deep)
        return remote(
            wbuf.at[source, span],
            wbuf.at[target, span],
            w_send.at[sends],
            w_recv.at[lands],
            where,
        )

    far_copies = [
        w_copy(y, 2 + y, piece, 0, 2 + piece, {"sp": far}) for piece in range(pieces)
    ]
    pass_copies = [w_copy(2 + y, 2 + y, piece, 2, 1, {"sp": side}) for piece in range(pieces)]
    for group, slot in enumerate((y, y, 2 + y)):
        all_sent(wbuf.at[slot], w_send.at[group])

    def pass_on(layer, point):
        for piece, turn in enumerate(PASS[layer]):
            if turn == point:
                far_copies[piece].wait_recv()
                pass_copies[piece].start()

    def w_pass(point):
        for layer in range(last + 1):
            if point in PASS[layer]:
                pl.when(z == layer)(functools.partial(pass_on, layer, point))

    def w_wait(block):
        ref = wbuf.at[2 * block + 1 - y]
        remote(ref, ref, w_send.at[0], w_recv.at[block], {"sp": side}).wait_recv()

    pltpu.make_async_copy(wbuf.at[y], wbuf.at[y], local_sem.at[1]).wait()
    def release(point):
        for piece in range(pieces):
            for layer in range(last + 1):
                if FAR[layer][piece] == point:
                    pl.when(z == layer)(far_copies[piece].start)
            if NEAR[piece] == point:
                w_copy(y, y, piece, 1, 0, {"sp": side}).start()

    release(0)

    @pl.when(y == 0)
    def _():
        kv[:, pl.ds(pl.multiple_of(side * rows, rows), rows), :] = jnp.zeros(
            (2, rows, kv.shape[2]), BF16
        )

    diagonal = lax.broadcasted_iota(jnp.int32, (rows, rows), 0) == lax.broadcasted_iota(
        jnp.int32, (rows, rows), 1
    )

    def to_lanes(column):
        return jnp.sum(jnp.where(diagonal, column, 0.0), axis=0, keepdims=True)

    def to_sublanes(row):
        return jnp.sum(jnp.where(diagonal, row, 0.0), axis=1, keepdims=True)

    load_gain.wait()
    gain = gain_v[...].astype(F32)[None, :]

    def norm_rows(slot):
        floats = tok[slot].astype(F32)
        scaled = floats * lax.rsqrt(jnp.mean(floats * floats, axis=-1, keepdims=True) + 1e-06)
        normed[pl.ds(pl.multiple_of(slot * rows_in, rows_in), rows_in), :] = (
            scaled * gain
        ).astype(BF16)

    def tok_wait(slot, lands):
        ref = tok.at[slot]
        remote(ref, ref, tok_send.at[0], tok_recv.at[lands], {"tp": core}).wait_recv()

    mid = rows // 2
    starts = [rem(t // 2 + part, 2) * mid for part in range(2)]

    def half_rows(part, offset=0):
        return pl.ds(pl.multiple_of(offset + starts[part], mid), mid)

    def project(weight, part):
        return jnp.dot(normed[half_rows(part), :], weight[...], preferred_element_type=F32)

    own_rows = pl.ds(pl.multiple_of(s * rows, rows), rows)

    def kv_copy(slot, part, sends, where):
        piece = kv.at[:, half_rows(part, slot * rows)]
        lands = n_sp + slot // 2 if where is side else 2 * (slot // 2) + part
        return remote(piece, piece, kv_send.at[sends], kv_recv.at[lands], {"sp": where})

    def kv_slot(slot):
        return kv.at[:, pl.ds(pl.multiple_of(slot * rows, rows), rows)]

    def kv_start(slot, part, sends, where, when):
        pl.when(when)(kv_copy(slot, part, sends, where).start)
        if part == 1:
            all_sent(kv_slot(slot), kv_send.at[sends], when)

    def kv_pass(distance, part, when):
        slot = rem(s + n_sp - 2 * distance, n_sp)
        pl.when(when)(kv_copy(slot, part, 0, up).wait_recv)
        if distance < last:
            kv_start(slot, part, 1 + 2 * distance, up, when & (z == last - 1))
        kv_start(slot, part, 2 + 2 * distance if distance < last else 7, side, when)

    def kv_own(part):
        both = project(wkv, part).astype(BF16)
        for column in range(2):
            kv[column, half_rows(part, s * rows), :] = both[
                :, column * kv_cols : (column + 1) * kv_cols
            ]
        kv_start(s, part, 1, up_two, z == 0)
        kv_start(s, part, 0, up, z < last)
        kv_start(s, part, 2, side, y == 0)

    rim = rim_out.shape[0]

    def glu_own(part):
        glu = project(wcv, part) * jax.nn.sigmoid(project(wcg, part))
        span = pl.ds(pl.multiple_of(rim + starts[part], rim), mid)
        pad[span, :] = glu.astype(BF16).astype(F32)

    def query_own(part):
        query[half_rows(part), :] = project(wq, part).astype(BF16)

    with scope("norm0"):
        norm_rows(t)
    with scope("tokw1"):
        tok_wait(core, 0)
    with scope("norm1"):
        norm_rows(core)
    with scope("kv0"):
        pltpu.make_async_copy(wkv, wkv, local_sem.at[4]).wait()
        kv_own(0)
    release(1)
    with scope("glu0"):
        load_cv.wait()
        load_cg.wait()
        glu_own(0)
    with scope("q0"):
        load_q.wait()
        query_own(0)
    with scope("tokw2"):
        for part in range(2):
            tok_copy(cross, part, 1, 1 + part, {"tp": cross}).wait_recv()
            tok_copy(cross, part, 2, 3, {"tp": core}).start()
    with scope("norm2"):
        norm_rows(cross)
    with scope("tokw3"):
        tok_wait(diag, 3)
    with scope("norm3"):
        norm_rows(diag)
    with scope("kv1"):
        kv_own(1)
    with scope("glu1"):
        glu_own(1)
        rim_out[...] = pad[pl.ds(rows, rim), :].astype(BF16)
    rim_copy = remote(rim_out, rim_in, rim_sem.at[0], rim_sem.at[1], {"sp": after})
    go(rim_copy)
    with scope("q1"):
        query_own(1)
    release(2)
    w_pass(2)
    with scope("kvp1"):
        for part in range(2):
            kv_pass(1, part, z >= 1)
        for part in range(2):
            kv_pass(2, part, z == last - 1)
    release(3)
    w_pass(3)
    with scope("rimw"):
        load_taps.wait()
        rim_copy.wait_recv()
    with scope("conv"):
        pad[pl.ds(0, rim), :] = jnp.where(s == 0, 0.0, rim_in[...].astype(F32))
        lead = rim - (KW - 1)
        conv = jnp.zeros((rows, ccols), F32)
        for tap in range(KW):
            conv = conv + taps[pl.ds(tap, 1), :].astype(F32) * pad[pl.ds(lead + tap, rows), :]
        stat[t] = jnp.zeros(stat.shape[1:], F32)
        stat[t, pl.ds(0, 1), :] = to_lanes(jnp.sum(conv, axis=1, keepdims=True))
        stat[t, pl.ds(1, 1), :] = to_lanes(jnp.sum(conv * conv, axis=1, keepdims=True))

    others = stat.at[pl.ds(0, n_tp - 1)]
    for peer in (core, cross, diag):
        remote(
            stat.at[t], stat.at[t], stat_send.at[0], stat_recv.at[0], {"tp": peer}
        ).start()
    all_sent(others, stat_send.at[0])
    release(4)
    with scope("kvp2"):
        for part in range(2):
            kv_pass(2, part, z == last)
        for part in range(2):
            kv_pass(3, part, z == last)
    with scope("wp0"):
        w_pass(4)
    def act_copy(first, size):
        span = pl.ds(first, size)
        return remote(
            act.at[0, :, span],
            act.at[1, :, span],
            act_send.at[0],
            act_recv.at[0],
            {"sp": mate},
        )

    act_copies = [act_copy(half, ccols)]
    act_copies += [act_copy(head * HEAD, HEAD) for head in range(head_count)]
    whole_act = act_copy(0, half + ccols)

    scale = 1.0 / math.sqrt(HEAD)

    def fold(first, past, states):
        span = pl.ds(first, past - first)
        spots = (rows, past - first)
        key_places = first + lax.broadcasted_iota(jnp.int32, spots, 1)
        allowed = key_places <= s * rows + lax.broadcasted_iota(jnp.int32, spots, 0)
        asked = jnp.concatenate(
            [query[:, head * HEAD : (head + 1) * HEAD] for head in range(head_count)], axis=0
        )
        scores = lax.dot_general(
            asked, kv[0, span], (((1,), (1,)), ((), ())), preferred_element_type=F32
        )
        tops, denoms, parts = [], [], []
        for head in range(head_count):
            query_gate = to_sublanes(gate[pl.ds(head, 1), own_rows])
            logits = (
                scores[head * rows : (head + 1) * rows] * scale
                + query_gate
                - gate[pl.ds(head, 1), span]
            )
            logits = jnp.where(allowed, logits, -1e30)
            top = jnp.max(logits, axis=-1, keepdims=True)
            if states is not None:
                top = jnp.maximum(top, states[head][0])
            weights = jnp.exp(logits - top)
            tops.append(top)
            denoms.append(jnp.sum(weights, axis=-1, keepdims=True))
            parts.append(weights.astype(BF16))
        product = jnp.dot(
            jnp.concatenate(parts, axis=0), kv[1, span], preferred_element_type=F32
        )
        result = []
        for head in range(head_count):
            denom, numer = denoms[head], product[head * rows : (head + 1) * rows]
            if states is not None:
                factor = jnp.exp(states[head][0] - tops[head])
                denom = denom + states[head][1] * factor
                numer = numer + states[head][2] * factor
            result.append((tops[head], denom, numer))
        return result

    def attend(layer):
        def arrive(distance):
            slot = rem(side + n_sp - 2 * distance, n_sp)
            ref = kv_slot(slot)
            copy = remote(
                ref, ref, kv_send.at[0], kv_recv.at[n_sp + slot // 2], {"sp": side}
            )
            pl.when(True if distance else y == 1)(copy.wait_recv)

        block = 2 * rows
        split = layer >= SPLIT_FROM
        for distance in range(layer + 1 - split):
            arrive(distance)
        load_gate.wait()
        states = fold(block * split, (layer + 1) * block, None)
        with scope("wpx"):
            pass_on(layer, 6)
        if split:
            arrive(layer)
            states = fold(0, block, states)
        for head in range(head_count):
            unused, denom, numer = states[head]
            act[0, :, pl.ds(head * HEAD, HEAD)] = (numer / denom).astype(BF16)
            act_copies[1 + head].start()

    for layer in range(AT_ONCE):

        @pl.when(z == layer)
        def _():
            with scope("attn_early"):
                attend(layer)

    release(5)
    with scope("statw"):
        load_cgain.wait()
        load_cbias.wait()
        remote(others, others, stat_send.at[0], stat_recv.at[0], {"tp": core}).wait_recv()

    with scope("convact"):
        totals = stat[0]
        for peer in range(1, n_tp):
            totals = totals + stat[peer]
        channels = n_tp * ccols
        mean_c = to_sublanes(totals[0:1]) / channels
        var_c = to_sublanes(totals[1:2]) / channels - mean_c * mean_c
        shaped = (conv - mean_c) * lax.rsqrt(var_c + 1e-05) * cgain_v[...].astype(F32)[
            None, :
        ] + cbias_v[...].astype(F32)[None, :]
        act[0, :, pl.ds(half, ccols)] = (shaped / (1.0 + jnp.exp(-shaped))).astype(BF16)
    act_copies[0].start()
    for layer in range(AT_ONCE, last + 1):

        @pl.when(z == layer)
        def _():
            with scope("attn_late"):
                attend(layer)

    sent.append((whole_act, None))
    with scope("wp1"):
        w_pass(7)
    with scope("wnear"):
        w_wait(0)

    def columns(part):
        return pl.ds(part * wide, wide)

    def product(row_set, block, part):
        return jnp.dot(
            act[row_set], wbuf[2 * block + part], preferred_element_type=F32
        )

    def pair_copy(row_set, part):
        return remote(
            pair_out.at[row_set, :, columns(part)],
            pair_in.at[row_set, :, columns(part)],
            pair_send.at[row_set],
            pair_recv.at[row_set, part],
            {"tp": core},
        )

    def ship(row_set, block):
        for part in range(2):
            pair_out[row_set, :, columns(part)] = product(row_set, block, part).astype(BF16)
            pair_copy(row_set, part).start()

    def keep(row_set, block):
        for part in range(2):
            acc[row_set, :, columns(part)] = product(row_set, block, part)

    def sum_copy(source, target, part, where):
        return remote(
            sum_out.at[source, :, columns(part)],
            sum_in.at[target, :, columns(part)],
            sum_send.at[source],
            sum_recv.at[target, part],
            where,
        )

    away = jnp.logical_not(home)
    own_sum = [sum_copy(0, 0, part, {"tp": cross}) for part in range(2)]
    mate_home = [sum_copy(1, 1, part, {"sp": mate}) for part in range(2)]
    mate_away = [sum_copy(1, 0, part, {"sp": mate, "tp": cross}) for part in range(2)]

    def finish(row_set):
        for part in range(2):
            pair_copy(row_set, part).wait_recv()
            total = acc[row_set, :, columns(part)] + pair_in[row_set, :, columns(part)].astype(F32)
            if row_set == 0:
                acc[0, :, columns(part)] = total
            sum_out[row_set, :, columns(part)] = total.astype(BF16)
            if row_set == 0:
                pl.when(away)(own_sum[part].start)
            else:
                pl.when(home)(mate_home[part].start)
                pl.when(away)(mate_away[part].start)

    def mate_wait():
        whole_act.wait_recv()

    def sums(mine, odd):
        with scope("a_near0"):
            if odd:
                mate_wait()
            for row_set in (1, 0) if odd else (0,):
                (keep if mine else ship)(row_set, 0)
        with scope("a_wfar"):
            w_wait(1)
        distant = ship if mine else keep
        if odd:
            with scope("a_mate"):
                distant(1, 1)
            if mine:
                distant(0, 1)
            with scope("a_fin1"):
                finish(1)
            if not mine:
                distant(0, 1)
            with scope("a_fin0"):
                finish(0)
        else:
            distant(0, 1)
            with scope("a_fin0"):
                finish(0)
            with scope("a_mate"):
                mate_wait()
            if mine:
                ship(1, 1)
                keep(1, 0)
            else:
                ship(1, 0)
                keep(1, 1)
            with scope("a_fin1"):
                finish(1)

    for odd in range(2):
        for mine in range(2):
            pl.when((rem(z, 2) == odd) & (near_mine if mine else jnp.logical_not(near_mine)))(
                functools.partial(sums, mine, odd)
            )

    @pl.when(home)
    def _():
        for part in range(2):
            with scope("c_home"):
                own_sum[part].wait_recv()
            span = columns(part)
            out_r[:, span] = (acc[0, :, span] + sum_in[0, :, span].astype(F32)).astype(BF16)

    @pl.when(away)
    def _():
        for part in range(2):
            with scope("c_away"):
                mate_home[part].wait_recv()
                mate_away[part].wait_recv()
            span = columns(part)
            out_r[:, span] = (
                sum_in[0, :, span].astype(F32) + sum_in[1, :, span].astype(F32)
            ).astype(BF16)

    for row_set in range(2):
        all_sent(pair_out.at[row_set], pair_send.at[row_set])
    all_sent(sum_out.at[0], sum_send.at[0], away)
    all_sent(sum_out.at[1], sum_send.at[1])
    with scope("sendw"):
        for copy, when in sent:
            if when is None:
                copy.wait_send()
            else:
                pl.when(when)(copy.wait_send)


def fused(n_sp, n_tp, *args):
    tokens, gain, wq, wk, wv, wcv, wcg, taps, cgain, cbias, gate, woa, woc = args
    rows_in, width = tokens.shape
    rows = rows_in * n_tp
    rim = -(-(KW - 1) // 16) * 16
    wide = woa.shape[1]
    out_wide = wide * n_sp // n_tp
    both = woa.shape[0] + woc.shape[0]
    pieces = 8
    hbm = pl.BlockSpec(memory_space=pltpu.HBM)
    vmem = pl.BlockSpec(memory_space=pltpu.VMEM)
    dma = pltpu.SemaphoreType.DMA
    scratch = [
        pltpu.VMEM((n_tp, rows_in, width), BF16),
        pltpu.VMEM((rows, width), BF16),
        pltpu.VMEM(wq.shape, BF16),
        pltpu.VMEM((width, wk.shape[1] + wv.shape[1]), BF16),
        *[pltpu.VMEM(w.shape, BF16) for w in (wcv, wcg, taps)],
        pltpu.VMEM(gate.shape[::-1], F32),
        pltpu.VMEM(gain.shape, BF16),
        pltpu.VMEM(cgain.shape, BF16),
        pltpu.VMEM(cbias.shape, BF16),
        pltpu.VMEM((4, both, wide), BF16),
        pltpu.VMEM((2, n_sp * rows, wk.shape[1]), BF16),
        pltpu.VMEM((rows, wq.shape[1]), BF16),
        pltpu.VMEM((rim + rows, wcv.shape[1]), F32),
        pltpu.VMEM((rim, wcv.shape[1]), BF16),
        pltpu.VMEM((rim, wcv.shape[1]), BF16),
        pltpu.VMEM((n_tp, 8, rows), F32),
        pltpu.VMEM((2, rows, both), BF16),
        pltpu.VMEM((2, rows, out_wide), F32),
        *[pltpu.VMEM((2, rows, out_wide), BF16)] * 4,
        dma((11,)),
        dma((3,)),
        dma((4,)),
        dma((3,)),
        dma((2 + pieces,)),
        dma((8,)),
        dma((n_sp + n_sp // 2,)),
        dma((2,)),
        *[dma((1,))] * 4,
        *[dma((2,)), dma((2, 2))] * 2,
    ]
    result = pltpu.VMEM((rows, out_wide), BF16)
    spare = 3 * rows * out_wide
    return pl.pallas_call(
        functools.partial(fused_kernel, n_sp, n_tp),
        out_shape=result,
        in_specs=[hbm] * 13,
        out_specs=vmem,
        scratch_shapes=scratch,
        compiler_params=pltpu.CompilerParams(
            collective_id=0, has_side_effects=True, vmem_limit_bytes=67_043_328 - spare
        ),
    )(
        tokens, gain, wq, wk, wv, wcv, wcg, taps,
        cgain, cbias, gate.T, woa, woc,
    )


def layer(sizes, *args):
    n_sp, n_tp = sizes["sp"], sizes["tp"]
    tokens, wq, wk, wcv, woa, woc = (args[k] for k in (0, 2, 3, 5, 11, 12))
    fits = (
        n_sp == 8
        and n_tp == 4
        and tokens.shape[0] * n_tp == HEAD
        and wk.shape[1] == HEAD
        and woa.shape[1] % HEAD == 0
        and woa.shape == woc.shape
        and wq.shape[1] == wcv.shape[1] == woa.shape[0]
    )
    if fits:
        return fused(n_sp, n_tp, *args)
    return shards(*args)


def solution(mesh):
    return jax.shard_map(
        functools.partial(layer, dict(mesh.shape)),
        mesh=mesh,
        in_specs=(
            P(("sp", "tp"), None),
            P(),
            P(None, "tp"),
            P(None, "tp"),
            P(None, "tp"),
            P(None, "tp"),
            P(None, "tp"),
            P(None, "tp"),
            P("tp"),
            P("tp"),
            P(None, "tp"),
            P("tp", "sp"),
            P("tp", "sp"),
        ),
        out_specs=P("sp", "tp"),
        check_vma=False,
    )
```
